32 devices in a mesh: sp: 4 (over z), dp: 8 (over y, x, core).
Axes of the slice: x: 2, y: 2, z: 4, core: 2. Of those that a mesh axis runs over, the one named last changes fastest.
Arguments:
- queries: bfloat16 [8, 768, 6144], P('dp', None, 'sp'), may hold values from -64 to 64
- out_grad: bfloat16 [8, 768, 4096], P('dp', None, 'sp'), may hold values from -6 to 6
- latent: bfloat16 [8, 768, 512], P('dp'), may hold values from -6 to 6
- rope_key: bfloat16 [8, 768, 64], P('dp'), may hold values from -6 to 6
- kv_gain: float32 [512], replicated, may hold values from 0.1 to 1.9
- key_up: bfloat16 [512, 4096], P('dp', 'sp'), may hold values from -0.25 to 0.25
- value_up: bfloat16 [512, 4096], P('dp', 'sp'), may hold values from -0.25 to 0.25
Outputs:
- query_grad: bfloat16 [8, 768, 6144], P('dp', None, 'sp')
- latent_grad: bfloat16 [8, 768, 512], P('dp')
- rope_key_grad: bfloat16 [8, 768, 64], P('dp')
- key_up_grad: float32 [512, 4096], P('dp', 'sp')
- value_up_grad: float32 [512, 4096], P('dp', 'sp')
The draws below stay inside these ranges and needn't reach their ends.
All inputs are finite; a program needn't handle non-finite values.
Results may differ from the reference program's by a relative error of at most 0.019.
The reference program's roundings to bfloat16 on the way count: a program that leaves them out, or rounds other values in their place, can miss the bound.
Values may be sent and summed in bfloat16 or wider, within the bound.
A program may use at most 64 MiB of HBM per device.

```python
import jax
import jax.numpy as jnp
from jax import lax

HEADS = 32
NOPE_DIM = 128
ROPE_DIM = 64
VALUE_DIM = 128
LATENT = 512
SEQ_LEN = 768
BATCH = 8
TOKENS = 6144
N_SP = 4


def draw_queries(key, part):
    shape = (BATCH, SEQ_LEN, HEADS * (NOPE_DIM + ROPE_DIM))
    base_key = jax.random.fold_in(key, 0)
    entries = jnp.clip(jax.random.normal(base_key, shape, jnp.float32), -6.0, 6.0)
    return entries.astype(jnp.bfloat16)


def shard_levels(stream_key, dims, pieces, smallest, high):
    level, own = 1.0, jax.random.fold_in(stream_key, 6)
    for dim, blocks in pieces:
        steps = jnp.exp(jax.random.uniform(jax.random.fold_in(own, dim), (blocks,), jnp.float32, smallest / len(pieces), high / len(pieces)))
        level = level * jnp.repeat(steps, dims[dim] // blocks).reshape([-1 if axis == dim else 1 for axis in range(len(dims))])
    return level


def normal_values(own_key, extent, scale, limit, shards=(), kind=jnp.bfloat16):
    result = jax.random.normal(own_key, extent, jnp.float32) * scale
    if len(shards) > 0:
        result = shard_levels(own_key, extent, shards, -0.22, 0.18) * result
    return jnp.clip(result, min=-limit, max=limit).astype(kind)


def setup_inputs(seed: int = 0) -> dict:
    splits = jax.random.split(jax.random.key(seed), 8)
    queries = draw_queries(jax.random.fold_in(splits[7], 71), 0)
    out_grad = normal_values(splits[1], (BATCH, SEQ_LEN, HEADS * VALUE_DIM), 1.0, 6.0, ((0, 8), (2, 4)))
    latent = normal_values(splits[2], (BATCH, SEQ_LEN, LATENT), 1.0, 6.0, ((0, 8),))
    rope_key = normal_values(splits[3], (BATCH, SEQ_LEN, ROPE_DIM), 1.0, 6.0, ((0, 8),))
    kv_gain = jnp.clip(1.0 + 0.18 * jax.random.normal(splits[4], (LATENT,), jnp.float32), 0.1, 1.9)
    key_up = normal_values(splits[5], (LATENT, HEADS * NOPE_DIM), LATENT ** -0.5, 0.25, ((0, 8), (1, 4)))
    value_up = normal_values(splits[6], (LATENT, HEADS * VALUE_DIM), LATENT ** -0.5, 0.25, ((0, 8), (1, 4)))
    return {"queries": queries, "out_grad": out_grad, "latent": latent, "rope_key": rope_key, "kv_gain": kv_gain, "key_up": key_up, "value_up": value_up}


norm_eps = 1e-06
rope_theta = 10000.0

def rope_tables(length, width):
    half_width = width // 2
    frequency = rope_theta ** (-(jnp.arange(half_width, dtype=jnp.float32) * 2.0 / width))
    position = jnp.arange(length, dtype=jnp.int32).astype(jnp.float32)
    angles = position[:, None] * frequency[None, :]
    return (jnp.cos(angles), jnp.sin(angles))

def rotate(tensor, cosine, sine_table):
    half_width = tensor.shape[-1] // 2
    first_half = tensor[..., :half_width]
    second = tensor[..., half_width:]
    return jnp.concatenate([first_half * cosine - second * sine_table, second * cosine + first_half * sine_table], axis=-1)

def unrotate(upstream, cosine, sine_table):
    half_width = upstream.shape[-1] // 2
    first_half = upstream[..., :half_width]
    second = upstream[..., half_width:]
    return jnp.concatenate([first_half * cosine + second * sine_table, second * cosine - first_half * sine_table], axis=-1)

def head_backward(query_used, key_used, head_value, head_grad, score_scale):
    length = query_used.shape[0]
    scores = jnp.dot(query_used, key_used.T, preferred_element_type=jnp.float32) * score_scale
    causal = lax.broadcasted_iota(jnp.int32, (length, length), 0) >= lax.broadcasted_iota(jnp.int32, (length, length), 1)
    scores = jnp.where(causal, scores, -jnp.inf)
    row_top = lax.optimization_barrier(jnp.max(scores, axis=1, keepdims=True))
    weights = jnp.exp(scores - row_top)
    probs = weights / lax.optimization_barrier(jnp.sum(weights, axis=1, keepdims=True))
    probs_low = probs.astype(jnp.bfloat16)
    value_grad = jnp.dot(probs_low.T, head_grad, preferred_element_type=jnp.float32).astype(jnp.bfloat16)
    prob_grad = jnp.dot(head_grad, head_value.T, preferred_element_type=jnp.float32)
    center = lax.optimization_barrier(jnp.sum(probs * prob_grad, axis=1, keepdims=True))
    score_grad = (probs * (prob_grad - center) * score_scale).astype(jnp.bfloat16)
    query_grad = jnp.dot(score_grad, key_used, preferred_element_type=jnp.float32)
    key_grad = jnp.dot(score_grad.T, query_used, preferred_element_type=jnp.float32)
    return (query_grad, key_grad, value_grad)

def attend(queries, head_grads, keys, values, key_rot, cosine, sine_table):
    length = queries.shape[0]
    head_count = head_grads.shape[1] // VALUE_DIM
    qk_width = NOPE_DIM + ROPE_DIM
    query_heads = queries.reshape(length, head_count, qk_width)
    rotated = rotate(query_heads[:, :, NOPE_DIM:].astype(jnp.float32), cosine[:, None, :], sine_table[:, None, :]).astype(jnp.bfloat16)
    query_used = jnp.concatenate([query_heads[:, :, :NOPE_DIM], rotated], axis=-1).transpose(1, 0, 2)
    key_heads = keys.reshape(length, head_count, NOPE_DIM).transpose(1, 0, 2)
    key_used = jnp.concatenate([key_heads, jnp.broadcast_to(key_rot[None], (head_count, length, ROPE_DIM))], axis=-1)
    value_heads = values.reshape(length, head_count, VALUE_DIM).transpose(1, 0, 2)
    grad_heads = head_grads.reshape(length, head_count, VALUE_DIM).transpose(1, 0, 2)
    score_scale = qk_width ** (-0.5)
    query_part, key_part, value_part = lax.map(lambda items: head_backward(items[0], items[1], items[2], items[3], score_scale), (query_used, key_used, value_heads, grad_heads))
    query_rot_grad = unrotate(query_part[:, :, NOPE_DIM:], cosine[None], sine_table[None])
    query_grad = jnp.concatenate([query_part[:, :, :NOPE_DIM], query_rot_grad], axis=-1).astype(jnp.bfloat16)
    query_grad = query_grad.transpose(1, 0, 2).reshape(length, head_count * qk_width)
    key_plain_grad = key_part[:, :, :NOPE_DIM].astype(jnp.bfloat16).transpose(1, 0, 2).reshape(length, head_count * NOPE_DIM)
    key_rot_grad = lax.optimization_barrier(jnp.sum(key_part[:, :, NOPE_DIM:], axis=0))
    value_grad = value_part.transpose(1, 0, 2).reshape(length, head_count * VALUE_DIM)
    return (query_grad, key_plain_grad, key_rot_grad, value_grad)

def finish(comp_total, rot_total, raw_latent, inverse, kv_gain, cosine, sine_table):
    mixed = comp_total * kv_gain
    spread = lax.optimization_barrier(jnp.mean(raw_latent * mixed, axis=-1, keepdims=True))
    latent_grad = (inverse * mixed - raw_latent * inverse ** 3 * spread).astype(jnp.bfloat16)
    rope_grad = unrotate(rot_total, cosine, sine_table).astype(jnp.bfloat16)
    return (latent_grad, rope_grad)

def reference(queries, out_grad, latent, rope_key, kv_gain, key_up, value_up):
    qk_width = NOPE_DIM + ROPE_DIM
    group = HEADS // N_SP
    cosine, sine_table = rope_tables(SEQ_LEN, ROPE_DIM)

    def one_sequence(totals, inputs):
        key_total, value_total = totals
        seq_queries, seq_grad, seq_latent, seq_rope = inputs
        raw_latent = seq_latent.astype(jnp.float32)
        inverse = lax.rsqrt(lax.optimization_barrier(jnp.mean(raw_latent * raw_latent, axis=-1, keepdims=True)) + norm_eps)
        compressed = (raw_latent * inverse * kv_gain).astype(jnp.bfloat16)
        key_rot = rotate(seq_rope.astype(jnp.float32), cosine, sine_table).astype(jnp.bfloat16)
        keys = jnp.dot(compressed, key_up, preferred_element_type=jnp.float32).astype(jnp.bfloat16)
        values = jnp.dot(compressed, value_up, preferred_element_type=jnp.float32).astype(jnp.bfloat16)

        def per_group(index):
            query_cols = lax.dynamic_slice_in_dim(seq_queries, index * (group * qk_width), group * qk_width, 1)
            grad_cols = lax.dynamic_slice_in_dim(seq_grad, index * (group * VALUE_DIM), group * VALUE_DIM, 1)
            key_cols = lax.dynamic_slice_in_dim(keys, index * (group * NOPE_DIM), group * NOPE_DIM, 1)
            value_cols = lax.dynamic_slice_in_dim(values, index * (group * VALUE_DIM), group * VALUE_DIM, 1)
            key_weight = lax.dynamic_slice_in_dim(key_up, index * (group * NOPE_DIM), group * NOPE_DIM, 1)
            value_weight = lax.dynamic_slice_in_dim(value_up, index * (group * VALUE_DIM), group * VALUE_DIM, 1)
            query_grad, key_plain_grad, key_rot_grad, value_grad = attend(query_cols, grad_cols, key_cols, value_cols, key_rot, cosine, sine_table)
            comp_part = jnp.dot(key_plain_grad, key_weight.T, preferred_element_type=jnp.float32) + jnp.dot(value_grad, value_weight.T, preferred_element_type=jnp.float32)
            return (query_grad, key_plain_grad, value_grad, comp_part, key_rot_grad)
        query_groups, key_groups, value_groups, comp_parts, rot_parts = lax.map(per_group, jnp.arange(N_SP, dtype=jnp.int32))
        query_grad = query_groups.transpose(1, 0, 2).reshape(SEQ_LEN, HEADS * qk_width)
        key_plain_all = key_groups.transpose(1, 0, 2).reshape(SEQ_LEN, HEADS * NOPE_DIM)
        value_all = value_groups.transpose(1, 0, 2).reshape(SEQ_LEN, HEADS * VALUE_DIM)
        comp_low = lax.optimization_barrier(comp_parts.astype(jnp.bfloat16))
        rot_low = lax.optimization_barrier(rot_parts.astype(jnp.bfloat16))
        comp_total = lax.optimization_barrier(jnp.sum(comp_low.astype(jnp.float32), axis=0))
        rot_total = lax.optimization_barrier(jnp.sum(rot_low.astype(jnp.float32), axis=0))
        latent_grad, rope_grad = finish(comp_total, rot_total, raw_latent, inverse, kv_gain, cosine, sine_table)
        contract = (((0,), (0,)), ((), ()))
        key_total = key_total + lax.dot_general(compressed, key_plain_all, contract, preferred_element_type=jnp.float32)
        value_total = value_total + lax.dot_general(compressed, value_all, contract, preferred_element_type=jnp.float32)
        return ((key_total, value_total), (query_grad, latent_grad, rope_grad))
    start_totals = (jnp.zeros((LATENT, HEADS * NOPE_DIM), jnp.float32), jnp.zeros((LATENT, HEADS * VALUE_DIM), jnp.float32))
    totals, outputs = lax.scan(one_sequence, start_totals, (queries, out_grad, latent, rope_key))
    grad_scale = float(TOKENS) ** (-0.5)
    return (outputs[0], outputs[1], outputs[2], totals[0] * grad_scale, totals[1] * grad_scale)
```

```python
import functools

import jax
import jax.numpy as jnp
import numpy as np
from jax import lax
from jax.experimental import pallas as pl
from jax.experimental.pallas import tpu as pltpu
from jax.sharding import PartitionSpec as P

NOPE_DIM = 128
ROPE_DIM = 64
VALUE_DIM = 128
QK = NOPE_DIM + ROPE_DIM
LOG2E = 1.4426950408889634

norm_eps = 1e-06
rope_theta = 10000.0

NT = (((1,), (1,)), ((), ()))
MESH = pl.DeviceIdType.MESH


def rope_tables(length):
    half = ROPE_DIM // 2
    frequency = np.float32(rope_theta) ** (-(np.arange(half, dtype=np.float32) * np.float32(2.0 / ROPE_DIM)))
    angles = np.arange(length, dtype=np.float32)[:, None] * frequency.astype(np.float32)[None, :]
    return np.cos(angles).astype(np.float32), np.sin(angles).astype(np.float32)


def dot(a, b):
    return jnp.dot(a, b, preferred_element_type=jnp.float32)


def dot_nt(a, b):
    return lax.dot_general(a, b, NT, preferred_element_type=jnp.float32)


def swap_halves(x):
    lane = lax.broadcasted_iota(jnp.int32, x.shape, 1)
    return jnp.where(lane % ROPE_DIM < ROPE_DIM // 2, pltpu.roll(x, 96, 1), pltpu.roll(x, 32, 1))


def each(first, count, act):
    def body(k, carry):
        act(k)
        return carry
    lax.fori_loop(first, count, body, 0)


def kernel(
    block, grad_scale, n_sp, n_dp,
    latent_hbm, rope_hbm, gain_hbm, cos_hbm, sin_hbm, cos_t_hbm, sin_t_hbm,
    q_hbm, do_hbm, wk_hbm, wv_hbm,
    dq_ref, grad_ref, low_ref,
    lat, rope, gain, cosw, sinw, cost, sint, qin, doin, w,
    comp, comp_t, krot, krot_t, ku, kt, vals, qu, pt, dst, dkv, acc, rot_acc,
    part, got_part, dwbuf, got_near, red, got_far,
    in_sem, w_sem, q_sem, do_sem,
    far_s, far_r, near_s, near_r, a_s, a_r, b_s, b_r, c_s, c_r, d_s, d_r,
):
    sp, dp = lax.axis_index("sp"), lax.axis_index("dp")
    chips = n_dp // 2
    chip, core = dp // 2, lax.rem(dp, 2)
    partner = chip * 2 + 1 - core
    pairs, length = qin.shape[0], qin.shape[1]
    width = lat.shape[1]
    tiles = length // block
    sub = block // n_sp
    scale = QK ** (-0.5)
    barrier = pltpu.get_barrier_semaphore()

    def chip_at(k):
        return lax.rem(chip + k, chips)

    def other(k):
        return chip_at(k) * 2 + core

    def source(k):
        return lax.rem(chip - k + chips, chips) * 2 + core

    def sp_peer(k):
        return lax.rem(sp + k, n_sp)

    def w_load(p, t):
        hbm = (wk_hbm, wv_hbm)[t]
        return pltpu.make_async_copy(
            hbm.at[:, pl.ds(pl.multiple_of(p * 256, 256), 256)],
            w.at[p, dp, :, pl.ds(t * 256, 256)], w_sem.at[p, t])

    for t in range(2):
        each(0, pairs, lambda p: w_load(p, t).start())
    each(1, chips, lambda k: pl.semaphore_signal(
        barrier, inc=1, device_id={"dp": other(k)}, device_id_type=MESH))
    each(1, n_sp, lambda k: pl.semaphore_signal(
        barrier, inc=1, device_id={"sp": sp_peer(k)}, device_id_type=MESH))
    pl.semaphore_signal(barrier, inc=1, device_id={"dp": partner}, device_id_type=MESH)

    loads = [
        pltpu.make_async_copy(src, dst_, in_sem.at[j]) for j, (src, dst_) in enumerate((
            (latent_hbm, lat), (gain_hbm, gain), (rope_hbm, rope), (cos_t_hbm, cost), (sin_t_hbm, sint),
            (cos_hbm, cosw), (sin_hbm, sinw)))]

    def q_load(p):
        return pltpu.make_async_copy(
            q_hbm.at[:, pl.ds(pl.multiple_of(p * 2 * QK, 128), 2 * QK)], qin.at[p], q_sem.at[p])

    def do_load(p):
        return pltpu.make_async_copy(
            do_hbm.at[:, pl.ds(pl.multiple_of(p * 256, 256), 256)], doin.at[p], do_sem.at[p])

    for copy in loads:
        copy.start()
    each(0, pairs, lambda p: q_load(p).start())
    each(0, pairs, lambda p: do_load(p).start())

    def far(p, k):
        return pltpu.make_async_remote_copy(
            src_ref=w.at[p, dp], dst_ref=w.at[p, dp],
            send_sem=far_s.at[p, k], recv_sem=far_r.at[p, k],
            device_id={"dp": other(k)}, device_id_type=MESH)

    def near(p, k):
        row = source(k)
        return pltpu.make_async_remote_copy(
            src_ref=w.at[p, row], dst_ref=w.at[p, row],
            send_sem=near_s.at[p, k], recv_sem=near_r.at[p, k],
            device_id={"dp": partner}, device_id_type=MESH)

    for t in range(2):
        each(0, pairs, lambda p: w_load(p, t).wait())
    pl.semaphore_wait(barrier, chips + n_sp - 1)

    def send_weights(p):
        each(1, chips, lambda k: far(p, k).start())
        near(p, 0).start()
    each(0, pairs, send_weights)

    def forward(p):
        def go(k):
            far(p, k).wait_recv()
            near(p, k).start()
        each(1, chips, go)

    for copy in loads:
        copy.wait()
    raw = lat[...].astype(jnp.float32)
    inverse = lax.rsqrt(jnp.mean(raw * raw, axis=-1, keepdims=True) + norm_eps)
    normed = raw * inverse * gain[...]
    comp[...] = normed.astype(jnp.bfloat16)
    comp_t[...] = normed.T.astype(jnp.bfloat16)
    ra = rope[:ROPE_DIM // 2, :].astype(jnp.float32)
    rb = rope[ROPE_DIM // 2:, :].astype(jnp.float32)
    turned = jnp.concatenate([ra * cost[...] - rb * sint[...], rb * cost[...] + ra * sint[...]], axis=0)
    krot_t[...] = turned.astype(jnp.bfloat16)
    krot[...] = jnp.concatenate([turned, turned], axis=0).T.astype(jnp.bfloat16)

    def turn_queries(p):
        q_load(p).wait()
        mid = qin[p, :, 128:256].astype(jnp.float32)
        last = qin[p, :, 256:384].astype(jnp.float32)
        low = lax.broadcasted_iota(jnp.int32, mid.shape, 1) < 64
        plain = jnp.where(low, pltpu.roll(mid, 64, 1), pltpu.roll(last, 64, 1))
        both = jnp.where(low, mid, last)
        rot = both * cosw[...] + swap_halves(both) * sinw[...]
        qu[2 * p, :, :NOPE_DIM] = qin[p, :, :128]
        qu[2 * p, :, NOPE_DIM:] = rot[:, :ROPE_DIM].astype(jnp.bfloat16)
        qu[2 * p + 1, :, :NOPE_DIM] = plain.astype(jnp.bfloat16)
        qu[2 * p + 1, :, NOPE_DIM:] = pltpu.roll(rot, 64, 1)[:, :ROPE_DIM].astype(jnp.bfloat16)
    each(0, pairs, turn_queries)
    each(0, pairs, lambda p: do_load(p).wait())

    def project(p):
        each(0, chips, lambda k: near(p, k).wait_recv())
        both = dot(comp[...], w[p].reshape(width, 512))
        keys = both[:, :256]
        keys_t = keys.T.astype(jnp.bfloat16)
        keys = keys.astype(jnp.bfloat16)
        vals[p] = both[:, 256:].astype(jnp.bfloat16)
        for h in range(2):
            ku[2 * p + h, :, :NOPE_DIM] = keys[:, h * NOPE_DIM:(h + 1) * NOPE_DIM]
            ku[2 * p + h, :, NOPE_DIM:] = krot[:, :ROPE_DIM]
            kt[2 * p + h, :NOPE_DIM, :] = keys_t[h * NOPE_DIM:(h + 1) * NOPE_DIM, :]
            kt[2 * p + h, NOPE_DIM:, :] = krot_t[...]

    def attend(i, p):
        rows = slice(i * block, (i + 1) * block)
        n = (i + 1) * block
        for h in range(2):
            cols = slice(h * VALUE_DIM, (h + 1) * VALUE_DIM)
            scores = dot_nt(ku[2 * p + h, :n, :], qu[2 * p + h, rows, :])
            key_at = lax.broadcasted_iota(jnp.int32, (block, block), 0)
            query_at = lax.broadcasted_iota(jnp.int32, (block, block), 1)
            diag = jnp.where(key_at <= query_at, scores[n - block:], -jnp.inf)
            scores = diag if i == 0 else jnp.concatenate([scores[:n - block], diag], axis=0)
            top = jnp.max(scores, axis=0, keepdims=True)
            e = jnp.exp2((scores - top) * (scale * LOG2E))
            r = 1.0 / jnp.sum(e, axis=0, keepdims=True)
            prob_grad = dot_nt(vals[p, :n, cols], doin[p, rows, cols])
            center = jnp.sum(e * prob_grad, axis=0, keepdims=True) * r
            pt[2 * p + h, :n, rows] = (e * r).astype(jnp.bfloat16)
            dst[2 * p + h, :n, rows] = (e * (r * scale) * (prob_grad - center)).astype(jnp.bfloat16)

    def key_block(i, p):
        rows = slice(i * block, (i + 1) * block)
        rot = None
        for h in range(2):
            cols = slice(h * VALUE_DIM, (h + 1) * VALUE_DIM)
            dv = dot(pt[2 * p + h, rows, i * block:], doin[p, i * block:, cols])
            dk = dot(dst[2 * p + h, rows, i * block:], qu[2 * p + h, i * block:, :])
            dkv[p, rows, h * NOPE_DIM:(h + 1) * NOPE_DIM] = dk[:, :NOPE_DIM].astype(jnp.bfloat16)
            dkv[p, rows, (2 + h) * 128:(3 + h) * 128] = dv.astype(jnp.bfloat16)
            rot = dk[:, NOPE_DIM:] if rot is None else rot + dk[:, NOPE_DIM:]
        rot_acc[...] += rot
        acc[...] += dot_nt(dkv[p, rows, :], w[p].reshape(width, 512))

    def part_copy(i, k):
        peer = sp_peer(k)
        return pltpu.make_async_remote_copy(
            src_ref=part.at[i, peer], dst_ref=got_part.at[i, k],
            send_sem=a_s.at[i, k], recv_sem=a_r.at[i, k],
            device_id={"sp": peer}, device_id_type=MESH)

    def low_copy(i, k):
        return pltpu.make_async_remote_copy(
            src_ref=low_ref.at[i, sp], dst_ref=low_ref.at[i, sp],
            send_sem=b_s.at[i, k], recv_sem=b_r.at[i, k],
            device_id={"sp": sp_peer(k)}, device_id_type=MESH)

    def send_part(i):
        rot = rot_acc[...].astype(jnp.bfloat16)
        whole = jnp.concatenate([acc[...].astype(jnp.bfloat16), rot, rot], axis=1)
        part[i] = whole.reshape(n_sp, sub, width + 128)
        each(1, n_sp, lambda k: part_copy(i, k).start())

    def finish(i):
        each(1, n_sp, lambda k: part_copy(i, k).wait())
        total = part[i, sp].astype(jnp.float32)
        for k in range(1, n_sp):
            total = total + got_part[i, k].astype(jnp.float32)
        mine = pl.ds(pl.multiple_of(i * block + sp * sub, sub), sub)
        raw = lat[mine, :].astype(jnp.float32)
        inverse = lax.rsqrt(jnp.mean(raw * raw, axis=-1, keepdims=True) + norm_eps)
        mixed = total[:, :width] * gain[...]
        spread = jnp.mean(raw * mixed, axis=-1, keepdims=True)
        low_ref[i, sp, :, :width] = (inverse * mixed - raw * inverse**3 * spread).astype(jnp.bfloat16)
        rot = total[:, width:]
        low_ref[i, sp, :, width:] = (
            rot * cosw[mine, :] - swap_halves(rot) * sinw[mine, :]
        ).astype(jnp.bfloat16)
        each(1, n_sp, lambda k: low_copy(i, k).start())

    def near_grad(p):
        return pltpu.make_async_remote_copy(
            src_ref=dwbuf.at[p, 1 - core], dst_ref=got_near.at[p],
            send_sem=c_s.at[p], recv_sem=c_r.at[p],
            device_id={"dp": partner}, device_id_type=MESH)

    def far_grad(p, k):
        return pltpu.make_async_remote_copy(
            src_ref=red.at[p, chip_at(k)], dst_ref=got_far.at[p, k],
            send_sem=d_s.at[p, k], recv_sem=d_r.at[p, k],
            device_id={"dp": other(k)}, device_id_type=MESH)

    def weight_grad(p):
        dw = dot(comp_t[...], dkv[p]) * grad_scale
        dw = dw.reshape(chips, 2, width // n_dp, 512)
        for c in range(2):
            dwbuf[p, c] = dw[:, c].astype(jnp.bfloat16)
        near_grad(p).start()

    def chip_grad(p):
        near_grad(p).wait_recv()
        both = dwbuf[p, core].astype(jnp.float32) + got_near[p].astype(jnp.float32)
        red[p] = both.astype(jnp.bfloat16)
        each(1, chips, lambda k: far_grad(p, k).start())

    def query_grad(i, p):
        rows = slice(i * block, (i + 1) * block)
        n = (i + 1) * block
        parts = []
        for h in range(2):
            g = dot(kt[2 * p + h, :, :n], dst[2 * p + h, :n, rows])
            a = g[NOPE_DIM:NOPE_DIM + 32]
            b = g[NOPE_DIM + 32:]
            c, s = cost[:, rows], sint[:, rows]
            parts += [g[:NOPE_DIM], a * c + b * s, b * c - a * s]
        dq_ref[rows, pl.ds(pl.multiple_of(p * 2 * QK, 128), 2 * QK)] = (
            jnp.concatenate(parts, axis=0).T.astype(jnp.bfloat16))

    forward(0)
    for i in reversed(range(tiles)):
        acc[...] = jnp.zeros_like(acc)
        rot_acc[...] = jnp.zeros_like(rot_acc)

        def step(p, i=i):
            if i == tiles - 1:
                project(p)
            attend(i, p)
            if i == tiles - 1:
                pl.when(p + 1 < pairs)(lambda: forward(p + 1))
            key_block(i, p)
        each(0, pairs, step)
        send_part(i)

    finish(tiles - 1)

    def grads(p):
        weight_grad(p)
        pl.when(p > 0)(lambda: chip_grad(p - 1))
    each(0, pairs, grads)
    chip_grad(pairs - 1)
    for i in range(tiles - 2, 0, -1):
        finish(i)

    for i in reversed(range(tiles)):
        each(0, pairs, lambda p, i=i: query_grad(i, p))

    if tiles > 1:
        finish(0)

    def add(p):
        total = red[p, chip].astype(jnp.float32)
        for k in range(1, chips):
            far_grad(p, k).wait()
            total = total + got_far[p, k].astype(jnp.float32)
        cols = pl.ds(pl.multiple_of(p * 256, 256), 256)
        grad_ref[0, :, cols] = total[:, :256]
        grad_ref[1, :, cols] = total[:, 256:]
        near_grad(p).wait_send()
        def drain(k):
            far(p, k).wait_send()
            near(p, k).wait_send()
        each(1, chips, drain)
        near(p, 0).wait_send()
    each(0, pairs, add)
    for i in range(tiles):
        each(1, n_sp, lambda k: low_copy(i, k).wait())


def fused(queries, out_grad, latent, rope_t, kv_gain, key_up, value_up, grad_scale, n_sp, n_dp):
    length, width = latent.shape
    pairs = key_up.shape[1] // 256
    heads = 2 * pairs
    chips = n_dp // 2
    block = 256
    tiles = length // block
    sub = block // n_sp
    depth = key_up.shape[0]
    cosine, sine = rope_tables(length)
    bf, f32 = jnp.bfloat16, jnp.float32
    hbm = pl.BlockSpec(memory_space=pl.ANY)
    vmem = pl.BlockSpec(memory_space=pltpu.VMEM)
    dma = lambda *n: pltpu.SemaphoreType.DMA(n)
    V = pltpu.VMEM
    return pl.pallas_call(
        functools.partial(kernel, block, grad_scale, n_sp, n_dp),
        in_specs=[hbm] * 11,
        out_specs=[vmem] * 3,
        out_shape=[
            jax.ShapeDtypeStruct(queries.shape, bf),
            jax.ShapeDtypeStruct((2, *key_up.shape), f32),
            jax.ShapeDtypeStruct((tiles, n_sp, sub, width + 128), bf),
        ],
        scratch_shapes=[
            V((length, width), bf), V((ROPE_DIM, length), bf), V((1, width), f32),
            V((length, 128), f32), V((length, 128), f32), V((32, length), f32), V((32, length), f32),
            V((pairs, length, 2 * QK), bf), V((pairs, length, 256), bf), V((pairs, n_dp, depth, 512), bf),
            V((length, width), bf), V((width, length), bf), V((length, 128), bf), V((ROPE_DIM, length), bf),
            V((heads, length, QK), bf), V((heads, QK, length), bf), V((pairs, length, 256), bf),
            V((heads, length, QK), bf), V((heads, length, length), bf), V((heads, length, length), bf),
            V((pairs, length, 512), bf), V((block, width), f32), V((block, ROPE_DIM), f32),
            V((tiles, n_sp, sub, width + 128), bf), V((tiles, n_sp, sub, width + 128), bf),
            V((pairs, 2, chips, depth, 512), bf), V((pairs, chips, depth, 512), bf),
            V((pairs, chips, depth, 512), bf), V((pairs, chips, depth, 512), bf),
            dma(7), dma(pairs, 2), dma(pairs), dma(pairs),
            dma(pairs, chips), dma(pairs, chips), dma(pairs, chips), dma(pairs, chips),
            dma(tiles, n_sp), dma(tiles, n_sp), dma(tiles, n_sp), dma(tiles, n_sp),
            dma(pairs), dma(pairs), dma(pairs, chips), dma(pairs, chips),
        ],
        compiler_params=pltpu.CompilerParams(
            collective_id=0, has_side_effects=True, vmem_limit_bytes=62 * 1024 * 1024
        ),
        name="fused_backward",
    )(
        latent, rope_t, kv_gain.reshape(1, -1), np.tile(cosine, (1, 4)),
        np.concatenate([-sine, sine, -sine, sine], axis=1),
        np.ascontiguousarray(cosine.T), np.ascontiguousarray(sine.T),
        queries, out_grad, key_up, value_up,
    )


def write_kernel(dq_ref, grad_ref, low_ref, dq_out, lat_out, rot_out, key_out, value_out, rot, sem):
    width = lat_out.shape[1]
    copies = [
        pltpu.make_async_copy(src, dst_, sem.at[j]) for j, (src, dst_) in enumerate((
            (dq_ref, dq_out), (low_ref.at[:, pl.ds(0, width)], lat_out),
            (grad_ref.at[0], key_out), (grad_ref.at[1], value_out), (rot, rot_out)))]
    for copy in copies[:4]:
        copy.start()
    rot[...] = low_ref[:, width:].astype(jnp.float32).T[:ROPE_DIM].astype(jnp.bfloat16)
    copies[4].start()
    for copy in copies:
        copy.wait()


def write(dq, grad, low):
    length, width = low.shape[0], low.shape[1] - 128
    bf, f32 = jnp.bfloat16, jnp.float32
    return pl.pallas_call(
        write_kernel,
        in_specs=[pl.BlockSpec(memory_space=pltpu.VMEM)] * 3,
        out_specs=[pl.BlockSpec(memory_space=pl.ANY)] * 5,
        out_shape=[
            jax.ShapeDtypeStruct(dq.shape, bf),
            jax.ShapeDtypeStruct((length, width), bf),
            jax.ShapeDtypeStruct((ROPE_DIM, length), bf),
            jax.ShapeDtypeStruct(grad.shape[1:], f32),
            jax.ShapeDtypeStruct(grad.shape[1:], f32),
        ],
        scratch_shapes=[pltpu.VMEM((ROPE_DIM, length), bf), pltpu.SemaphoreType.DMA((5,))],
        compiler_params=pltpu.CompilerParams(vmem_limit_bytes=16 * 1024 * 1024),
        name="write_outputs",
    )(dq, grad, low)


def shards(queries, out_grad, latent, rope_key, kv_gain, key_up, value_up):
    length, width = latent.shape[1:]
    n_sp, n_dp = lax.axis_size("sp"), lax.axis_size("dp")
    grad_scale = float(n_dp * length) ** (-0.5)
    rope_t = jnp.swapaxes(rope_key, 1, 2)[0]
    dq, grad, low = fused(
        queries[0], out_grad[0], latent[0], rope_t, kv_gain, key_up, value_up, grad_scale, n_sp, n_dp
    )
    dq, lat, rot_t, key_grad, value_grad = write(dq, grad, low.reshape(length, width + 128))
    return dq[None], lat[None], jnp.swapaxes(rot_t[None], 1, 2), key_grad, value_grad


def solution(mesh):
    return jax.shard_map(
        shards,
        mesh=mesh,
        in_specs=(
            P("dp", None, "sp"),
            P("dp", None, "sp"),
            P("dp", None, None),
            P("dp", None, None),
            P(),
            P("dp", "sp"),
            P("dp", "sp"),
        ),
        out_specs=(
            P("dp", None, "sp"),
            P("dp", None, None),
            P("dp", None, None),
            P("dp", "sp"),
            P("dp", "sp"),
        ),
        check_vma=False,
    )
```

```python
import functools

import jax
import jax.numpy as jnp
import numpy as np
from jax import lax
from jax.experimental import pallas as pl
from jax.experimental.pallas import tpu as pltpu
from jax.sharding import PartitionSpec as P

NOPE_DIM = 128
ROPE_DIM = 64
VALUE_DIM = 128
QK = NOPE_DIM + ROPE_DIM
LOG2E = 1.4426950408889634

norm_eps = 1e-06
rope_theta = 10000.0

NT = (((1,), (1,)), ((), ()))
MESH = pl.DeviceIdType.MESH


def rope_tables(length):
    half = ROPE_DIM // 2
    frequency = np.float32(rope_theta) ** (-(np.arange(half, dtype=np.float32) * np.float32(2.0 / ROPE_DIM)))
    angles = np.arange(length, dtype=np.float32)[:, None] * frequency.astype(np.float32)[None, :]
    return np.cos(angles).astype(np.float32), np.sin(angles).astype(np.float32)


def dot(a, b):
    return jnp.dot(a, b, preferred_element_type=jnp.float32)


def dot_nt(a, b):
    return lax.dot_general(a, b, NT, preferred_element_type=jnp.float32)


def swap_halves(x):
    lane = lax.broadcasted_iota(jnp.int32, x.shape, 1)
    return jnp.where(lane % ROPE_DIM < ROPE_DIM // 2, pltpu.roll(x, 96, 1), pltpu.roll(x, 32, 1))


def each(first, count, act):
    def body(k, carry):
        act(k)
        return carry
    lax.fori_loop(first, count, body, 0)


def kernel(
    block, grad_scale, n_sp, n_dp,
    latent_hbm, rope_hbm, gain_hbm, cos_hbm, sin_hbm, cos_t_hbm, sin_t_hbm,
    q_hbm, do_hbm, wk_hbm, wv_hbm,
    dq_ref, grad_ref, low_ref,
    lat, rope, gain, cosw, sinw, cost, sint, qin, doin, w,
    comp, comp_t, krot, krot_t, ku, kt, vals, qu, pt, dst, dkv, acc, rot_acc,
    part, got_in, got_mid, dwbuf, got_near, red, got_far,
    in_sem, w_sem, q_sem, do_sem,
    far_s, far_r, near_s, near_r, a_s, a_r, m_s, m_r, b_s, b_r, c_s, c_r, d_s, d_r,
):
    sp, dp = lax.axis_index("sp"), lax.axis_index("dp")
    chips = n_dp // 2
    chip, core = dp // 2, lax.rem(dp, 2)
    partner = chip * 2 + 1 - core
    pairs, length = qin.shape[0], qin.shape[1]
    width = lat.shape[1]
    tiles = length // block
    pieces = part.shape[1]
    rows_of = block // pieces
    scale = QK ** (-0.5)
    barrier = pltpu.get_barrier_semaphore()

    def chip_at(k):
        return lax.rem(chip + k, chips)

    def other(k):
        return chip_at(k) * 2 + core

    def source(k):
        return lax.rem(chip - k + chips, chips) * 2 + core

    def w_load(p, t):
        hbm = (wk_hbm, wv_hbm)[t]
        return pltpu.make_async_copy(
            hbm.at[:, pl.ds(pl.multiple_of(p * 256, 256), 256)],
            w.at[p, dp, :, pl.ds(t * 256, 256)], w_sem.at[p, t])

    for t in range(2):
        each(0, pairs, lambda p: w_load(p, t).start())
    each(1, chips, lambda k: pl.semaphore_signal(
        barrier, inc=1, device_id={"dp": other(k)}, device_id_type=MESH))
    lower = sp < n_sp // 2
    at_end = jnp.logical_or(sp == 0, sp == n_sp - 1)
    at_middle = jnp.logical_or(sp == n_sp // 2 - 1, sp == n_sp // 2)
    inward = jnp.where(lower, sp + 1, sp - 1)
    outward = jnp.where(lower, sp - 1, sp + 1)
    pl.semaphore_signal(barrier, inc=1, device_id={"sp": inward}, device_id_type=MESH)
    pl.when(jnp.logical_not(at_end))(lambda: pl.semaphore_signal(
        barrier, inc=1, device_id={"sp": outward}, device_id_type=MESH))
    pl.semaphore_signal(barrier, inc=1, device_id={"dp": partner}, device_id_type=MESH)

    loads = [
        pltpu.make_async_copy(src, dst_, in_sem.at[j]) for j, (src, dst_) in enumerate((
            (latent_hbm, lat), (gain_hbm, gain), (rope_hbm, rope), (cos_t_hbm, cost), (sin_t_hbm, sint),
            (cos_hbm, cosw), (sin_hbm, sinw)))]

    def q_load(p):
        return pltpu.make_async_copy(
            q_hbm.at[:, pl.ds(pl.multiple_of(p * 2 * QK, 128), 2 * QK)], qin.at[p], q_sem.at[p])

    def do_load(p):
        return pltpu.make_async_copy(
            do_hbm.at[:, pl.ds(pl.multiple_of(p * 256, 256), 256)], doin.at[p], do_sem.at[p])

    for copy in loads:
        copy.start()
    each(0, pairs, lambda p: q_load(p).start())
    each(0, pairs, lambda p: do_load(p).start())

    def far(p, k):
        return pltpu.make_async_remote_copy(
            src_ref=w.at[p, dp], dst_ref=w.at[p, dp],
            send_sem=far_s.at[p, k], recv_sem=far_r.at[p, k],
            device_id={"dp": other(k)}, device_id_type=MESH)

    def near(p, k):
        row = source(k)
        return pltpu.make_async_remote_copy(
            src_ref=w.at[p, row], dst_ref=w.at[p, row],
            send_sem=near_s.at[p, k], recv_sem=near_r.at[p, k],
            device_id={"dp": partner}, device_id_type=MESH)

    for t in range(2):
        each(0, pairs, lambda p: w_load(p, t).wait())
    pl.semaphore_wait(barrier, chips + jnp.where(at_end, 1, 2))

    def send_weights(p):
        each(1, chips, lambda k: far(p, k).start())
        near(p, 0).start()
    each(0, pairs, send_weights)

    def forward(p):
        def go(k):
            far(p, k).wait_recv()
            near(p, k).start()
        each(1, chips, go)

    for copy in loads:
        copy.wait()
    raw = lat[...].astype(jnp.float32)
    inverse = lax.rsqrt(jnp.mean(raw * raw, axis=-1, keepdims=True) + norm_eps)
    normed = raw * inverse * gain[...]
    comp[...] = normed.astype(jnp.bfloat16)
    comp_t[...] = normed.T.astype(jnp.bfloat16)
    ra = rope[:ROPE_DIM // 2, :].astype(jnp.float32)
    rb = rope[ROPE_DIM // 2:, :].astype(jnp.float32)
    turned = jnp.concatenate([ra * cost[...] - rb * sint[...], rb * cost[...] + ra * sint[...]], axis=0)
    krot_t[...] = turned.astype(jnp.bfloat16)
    krot[...] = jnp.concatenate([turned, turned], axis=0).T.astype(jnp.bfloat16)

    def turn_queries(p):
        q_load(p).wait()
        mid = qin[p, :, 128:256].astype(jnp.float32)
        last = qin[p, :, 256:384].astype(jnp.float32)
        low = lax.broadcasted_iota(jnp.int32, mid.shape, 1) < 64
        plain = jnp.where(low, pltpu.roll(mid, 64, 1), pltpu.roll(last, 64, 1))
        both = jnp.where(low, mid, last)
        rot = both * cosw[...] + swap_halves(both) * sinw[...]
        qu[2 * p, :, :NOPE_DIM] = qin[p, :, :128]
        qu[2 * p, :, NOPE_DIM:] = rot[:, :ROPE_DIM].astype(jnp.bfloat16)
        qu[2 * p + 1, :, :NOPE_DIM] = plain.astype(jnp.bfloat16)
        qu[2 * p + 1, :, NOPE_DIM:] = pltpu.roll(rot, 64, 1)[:, :ROPE_DIM].astype(jnp.bfloat16)
    each(0, pairs, turn_queries)
    each(0, pairs, lambda p: do_load(p).wait())

    def project(p):
        each(0, chips, lambda k: near(p, k).wait_recv())
        both = dot(comp[...], w[p].reshape(width, 512))
        keys = both[:, :256]
        keys_t = keys.T.astype(jnp.bfloat16)
        keys = keys.astype(jnp.bfloat16)
        vals[p] = both[:, 256:].astype(jnp.bfloat16)
        for h in range(2):
            ku[2 * p + h, :, :NOPE_DIM] = keys[:, h * NOPE_DIM:(h + 1) * NOPE_DIM]
            ku[2 * p + h, :, NOPE_DIM:] = krot[:, :ROPE_DIM]
            kt[2 * p + h, :NOPE_DIM, :] = keys_t[h * NOPE_DIM:(h + 1) * NOPE_DIM, :]
            kt[2 * p + h, NOPE_DIM:, :] = krot_t[...]

    def attend(i, p):
        rows = slice(i * block, (i + 1) * block)
        n = (i + 1) * block
        for h in range(2):
            cols = slice(h * VALUE_DIM, (h + 1) * VALUE_DIM)
            scores = dot_nt(ku[2 * p + h, :n, :], qu[2 * p + h, rows, :])
            key_at = lax.broadcasted_iota(jnp.int32, (block, block), 0)
            query_at = lax.broadcasted_iota(jnp.int32, (block, block), 1)
            diag = jnp.where(key_at <= query_at, scores[n - block:], -jnp.inf)
            scores = diag if i == 0 else jnp.concatenate([scores[:n - block], diag], axis=0)
            top = jnp.max(scores, axis=0, keepdims=True)
            e = jnp.exp2((scores - top) * (scale * LOG2E))
            r = 1.0 / jnp.sum(e, axis=0, keepdims=True)
            prob_grad = dot_nt(vals[p, :n, cols], doin[p, rows, cols])
            center = jnp.sum(e * prob_grad, axis=0, keepdims=True) * r
            prob = (e * r).astype(jnp.bfloat16)
            grad = (e * (r * scale) * (prob_grad - center)).astype(jnp.bfloat16)
            for j in range(i + 1):
                at = slice((i - j) * block, (i - j + 1) * block)
                pt[j][2 * p + h, :, at] = prob[j * block:(j + 1) * block]
                dst[j][2 * p + h, :, at] = grad[j * block:(j + 1) * block]

    def key_block(i, p):
        rows = slice(i * block, (i + 1) * block)
        rot = None
        for h in range(2):
            cols = slice(h * VALUE_DIM, (h + 1) * VALUE_DIM)
            dv = dot(pt[i][2 * p + h], doin[p, i * block:, cols])
            dk = dot(dst[i][2 * p + h], qu[2 * p + h, i * block:, :])
            dkv[p, rows, h * NOPE_DIM:(h + 1) * NOPE_DIM] = dk[:, :NOPE_DIM].astype(jnp.bfloat16)
            dkv[p, rows, (2 + h) * 128:(3 + h) * 128] = dv.astype(jnp.bfloat16)
            rot = dk[:, NOPE_DIM:] if rot is None else rot + dk[:, NOPE_DIM:]
        rot_acc[...] += rot
        acc[...] += dot_nt(dkv[p, rows, :], w[p].reshape(width, 512))

    def in_copy(i, q):
        return pltpu.make_async_remote_copy(
            src_ref=part.at[i, q], dst_ref=got_in.at[i, q],
            send_sem=a_s.at[i, q], recv_sem=a_r.at[i, q],
            device_id={"sp": inward}, device_id_type=MESH)

    def mid_copy(i, q):
        return pltpu.make_async_remote_copy(
            src_ref=part.at[i, q], dst_ref=got_mid.at[i, q],
            send_sem=m_s.at[i, q], recv_sem=m_r.at[i, q],
            device_id={"sp": inward}, device_id_type=MESH)

    def out_copy(i, q):
        return pltpu.make_async_remote_copy(
            src_ref=low_ref.at[i, q], dst_ref=low_ref.at[i, q],
            send_sem=b_s.at[i, q], recv_sem=b_r.at[i, q],
            device_id={"sp": outward}, device_id_type=MESH)

    def go_in(i, q):
        pl.when(at_middle)(lambda: mid_copy(i, q).start())
        pl.when(jnp.logical_not(at_middle))(lambda: in_copy(i, q).start())

    def send_part(i):
        rot = rot_acc[...].astype(jnp.bfloat16)
        whole = jnp.concatenate([acc[...].astype(jnp.bfloat16), rot, rot], axis=1)
        part[i] = whole.reshape(pieces, rows_of, width + 128)
        def go():
            for q in range(pieces):
                go_in(i, q)
        pl.when(at_end)(go)

    def merge(i, q):
        def go():
            in_copy(i, q).wait_recv()
            part[i, q] = (part[i, q].astype(jnp.float32) + got_in[i, q].astype(jnp.float32)).astype(jnp.bfloat16)
            go_in(i, q)
        pl.when(jnp.logical_not(at_end))(go)

    def finish(i, q):
        def go():
            mid_copy(i, q).wait_recv()
            total = part[i, q].astype(jnp.float32) + got_mid[i, q].astype(jnp.float32)
            mine = slice(i * block + q * rows_of, i * block + (q + 1) * rows_of)
            raw = lat[mine, :].astype(jnp.float32)
            inverse = lax.rsqrt(jnp.mean(raw * raw, axis=-1, keepdims=True) + norm_eps)
            mixed = total[:, :width] * gain[...]
            spread = jnp.mean(raw * mixed, axis=-1, keepdims=True)
            low_ref[i, q, :, :width] = (inverse * mixed - raw * inverse**3 * spread).astype(jnp.bfloat16)
            rot = total[:, width:]
            low_ref[i, q, :, width:] = (
                rot * cosw[mine, :] - swap_halves(rot) * sinw[mine, :]
            ).astype(jnp.bfloat16)
            pl.when(jnp.logical_not(at_end))(lambda: out_copy(i, q).start())
        pl.when(at_middle)(go)

    def deliver(i, q):
        def go():
            out_copy(i, q).wait_recv()
            pl.when(jnp.logical_not(at_end))(lambda: out_copy(i, q).start())
        pl.when(jnp.logical_not(at_middle))(go)

    def drain_rows(i, q):
        pl.when(at_middle)(lambda: mid_copy(i, q).wait_send())
        pl.when(jnp.logical_not(at_middle))(lambda: in_copy(i, q).wait_send())
        pl.when(jnp.logical_not(at_end))(lambda: out_copy(i, q).wait_send())

    def near_grad(p):
        return pltpu.make_async_remote_copy(
            src_ref=dwbuf.at[p, 1 - core], dst_ref=got_near.at[p],
            send_sem=c_s.at[p], recv_sem=c_r.at[p],
            device_id={"dp": partner}, device_id_type=MESH)

    def far_grad(p, k):
        return pltpu.make_async_remote_copy(
            src_ref=red.at[p, chip_at(k)], dst_ref=got_far.at[p, k],
            send_sem=d_s.at[p, k], recv_sem=d_r.at[p, k],
            device_id={"dp": other(k)}, device_id_type=MESH)

    def weight_grad(p):
        dw = dot(comp_t[...], dkv[p]) * grad_scale
        dw = dw.reshape(chips, 2, width // n_dp, 512)
        for c in range(2):
            dwbuf[p, c] = dw[:, c].astype(jnp.bfloat16)
        near_grad(p).start()

    def chip_grad(p):
        near_grad(p).wait_recv()
        both = dwbuf[p, core].astype(jnp.float32) + got_near[p].astype(jnp.float32)
        red[p] = both.astype(jnp.bfloat16)
        each(1, chips, lambda k: far_grad(p, k).start())

    def query_grad(i, p):
        rows = slice(i * block, (i + 1) * block)
        n = (i + 1) * block
        parts = []
        for h in range(2):
            g = dot(kt[2 * p + h, :, :n], jnp.concatenate(
                [dst[j][2 * p + h, :, (i - j) * block:(i - j + 1) * block] for j in range(i + 1)], axis=0))
            a = g[NOPE_DIM:NOPE_DIM + 32]
            b = g[NOPE_DIM + 32:]
            c, s = cost[:, rows], sint[:, rows]
            parts += [g[:NOPE_DIM], a * c + b * s, b * c - a * s]
        dq_ref[rows, pl.ds(pl.multiple_of(p * 2 * QK, 128), 2 * QK)] = (
            jnp.concatenate(parts, axis=0).T.astype(jnp.bfloat16))

    last = pairs - 1
    stages = {}

    def stage(act, i, *keys):
        for q, key in enumerate(keys):
            phase, at = key if isinstance(key, tuple) else (key, None)
            key = phase if at is None else (phase, min(at, last))
            stages.setdefault(key, []).append(functools.partial(act, i, q))

    for i in range(tiles - 1, 0, -1):
        if i > 1:
            stage(merge, i, (i - 1, 2), (i - 1, 3), ("sent", i - 1), (i - 2, 0))
            stage(finish, i, (i - 2, 0), (i - 2, 1), (i - 2, 2), (i - 2, 3))
        else:
            stage(merge, 1, (0, 2), (0, 3), ("w", 1), ("w", 3))
            stage(finish, 1, ("w", 3), "grads", ("q2", 2), ("q1", 1))
    stage(merge, 0, ("q2", 2), ("q1", 2), "end", "end3")
    stage(finish, 0, "end1", "end4", "end5", "end6")

    def run(key):
        for act in stages.pop(key, []):
            act()

    def run_in(name, p):
        for at in range(pairs):
            if (name, at) in stages:
                pl.when(p == at)(functools.partial(run, (name, at)))

    forward(0)
    for i in reversed(range(tiles)):
        acc[...] = jnp.zeros_like(acc)
        rot_acc[...] = jnp.zeros_like(rot_acc)

        def step(p, i=i):
            if i == tiles - 1:
                project(p)
            attend(i, p)
            if i == tiles - 1:
                pl.when(p + 1 < pairs)(lambda: forward(p + 1))
            key_block(i, p)
            run_in(i, p)
        each(0, pairs, step)
        send_part(i)
        run(("sent", min(i, last)))

    def grads(p):
        weight_grad(p)
        pl.when(p > 0)(lambda: chip_grad(p - 1))
        run_in("w", p)
    each(0, pairs, grads)
    chip_grad(pairs - 1)
    run("grads")

    for i in reversed(range(tiles)):
        def turn_back(p, i=i):
            query_grad(i, p)
            run_in("q" + str(i), p)
        each(0, pairs, turn_back)
    for key in sorted(k for k in stages if isinstance(k, str)):
        run(key)
    assert not stages

    def add(p):
        total = red[p, chip].astype(jnp.float32)
        for k in range(1, chips):
            far_grad(p, k).wait()
            total = total + got_far[p, k].astype(jnp.float32)
        cols = pl.ds(pl.multiple_of(p * 256, 256), 256)
        grad_ref[0, :, cols] = total[:, :256]
        grad_ref[1, :, cols] = total[:, 256:]
        near_grad(p).wait_send()
        def drain(k):
            far(p, k).wait_send()
            near(p, k).wait_send()
        each(1, chips, drain)
        near(p, 0).wait_send()
    each(0, pairs, add)
    for i in reversed(range(tiles)):
        for q in range(pieces):
            deliver(i, q)
            drain_rows(i, q)


def fused(queries, out_grad, latent, rope_t, kv_gain, key_up, value_up, grad_scale, n_sp, n_dp):
    length, width = latent.shape
    pairs = key_up.shape[1] // 256
    heads = 2 * pairs
    chips = n_dp // 2
    block = 256
    tiles = length // block
    pieces = 4
    piece = (tiles, pieces, block // pieces, width + 128)
    depth = key_up.shape[0]
    cosine, sine = rope_tables(length)
    bf, f32 = jnp.bfloat16, jnp.float32
    hbm = pl.BlockSpec(memory_space=pltpu.HBM)
    vmem = pl.BlockSpec(memory_space=pltpu.VMEM)
    dma = lambda *n: pltpu.SemaphoreType.DMA(n)
    V = pltpu.VMEM
    triangle = tuple(V((heads, block, length - j * block), bf) for j in range(tiles))
    return pl.pallas_call(
        functools.partial(kernel, block, grad_scale, n_sp, n_dp),
        in_specs=[hbm] * 11,
        out_specs=[vmem] * 3,
        out_shape=[
            jax.ShapeDtypeStruct(queries.shape, bf),
            jax.ShapeDtypeStruct((2, *key_up.shape), f32),
            jax.ShapeDtypeStruct(piece, bf),
        ],
        scratch_shapes=[
            V((length, width), bf), V((ROPE_DIM, length), bf), V((1, width), f32),
            V((length, 128), f32), V((length, 128), f32), V((32, length), f32), V((32, length), f32),
            V((pairs, length, 2 * QK), bf), V((pairs, length, 256), bf), V((pairs, n_dp, depth, 512), bf),
            V((length, width), bf), V((width, length), bf), V((length, 128), bf), V((ROPE_DIM, length), bf),
            V((heads, length, QK), bf), V((heads, QK, length), bf), V((pairs, length, 256), bf),
            V((heads, length, QK), bf), triangle, triangle,
            V((pairs, length, 512), bf), V((block, width), f32), V((block, ROPE_DIM), f32),
            V(piece, bf), V(piece, bf), V(piece, bf),
            V((pairs, 2, chips, depth, 512), bf), V((pairs, chips, depth, 512), bf),
            V((pairs, chips, depth, 512), bf), V((pairs, chips, depth, 512), bf),
            dma(7), dma(pairs, 2), dma(pairs), dma(pairs),
            dma(pairs, chips), dma(pairs, chips), dma(pairs, chips), dma(pairs, chips),
            *[dma(tiles, pieces)] * 6,
            dma(pairs), dma(pairs), dma(pairs, chips), dma(pairs, chips),
        ],
        compiler_params=pltpu.CompilerParams(
            collective_id=0, has_side_effects=True, vmem_limit_bytes=50 * 1024 * 1024
        ),
        name="fused_backward",
    )(*(pltpu.with_memory_space_constraint(jnp.asarray(x), pltpu.HBM) for x in (
        latent, rope_t, kv_gain.reshape(1, -1), np.tile(cosine, (1, 4)),
        np.concatenate([-sine, sine, -sine, sine], axis=1),
        np.ascontiguousarray(cosine.T), np.ascontiguousarray(sine.T),
        queries, out_grad, key_up, value_up,
    )))


def write_kernel(dq_ref, grad_ref, low_ref, dq_out, lat_out, rot_out, key_out, value_out, rot, sem):
    width = lat_out.shape[1]
    copies = [
        pltpu.make_async_copy(src, dst_, sem.at[j]) for j, (src, dst_) in enumerate((
            (dq_ref, dq_out), (low_ref.at[:, pl.ds(0, width)], lat_out),
            (grad_ref.at[0], key_out), (grad_ref.at[1], value_out), (rot, rot_out)))]
    for copy in copies[:4]:
        copy.start()
    rot[...] = low_ref[:, width:].astype(jnp.float32).T[:ROPE_DIM].astype(jnp.bfloat16)
    copies[4].start()
    for copy in copies:
        copy.wait()


def write(dq, grad, low):
    length, width = low.shape[0], low.shape[1] - 128
    bf, f32 = jnp.bfloat16, jnp.float32
    return pl.pallas_call(
        write_kernel,
        in_specs=[pl.BlockSpec(memory_space=pltpu.VMEM)] * 3,
        out_specs=[pl.BlockSpec(memory_space=pl.ANY)] * 5,
        out_shape=[
            jax.ShapeDtypeStruct(dq.shape, bf),
            jax.ShapeDtypeStruct((length, width), bf),
            jax.ShapeDtypeStruct((ROPE_DIM, length), bf),
            jax.ShapeDtypeStruct(grad.shape[1:], f32),
            jax.ShapeDtypeStruct(grad.shape[1:], f32),
        ],
        scratch_shapes=[pltpu.VMEM((ROPE_DIM, length), bf), pltpu.SemaphoreType.DMA((5,))],
        compiler_params=pltpu.CompilerParams(vmem_limit_bytes=16 * 1024 * 1024),
        name="write_outputs",
    )(dq, grad, low)


def shards(queries, out_grad, latent, rope_key, kv_gain, key_up, value_up):
    length, width = latent.shape[1:]
    n_sp, n_dp = lax.axis_size("sp"), lax.axis_size("dp")
    grad_scale = float(n_dp * length) ** (-0.5)
    rope_t = jnp.swapaxes(rope_key, 1, 2)[0]
    dq, grad, low = fused(
        queries[0], out_grad[0], latent[0], rope_t, kv_gain, key_up, value_up, grad_scale, n_sp, n_dp
    )
    dq, lat, rot_t, key_grad, value_grad = write(dq, grad, low.reshape(length, width + 128))
    return dq[None], lat[None], jnp.swapaxes(rot_t[None], 1, 2), key_grad, value_grad


def solution(mesh):
    return jax.shard_map(
        shards,
        mesh=mesh,
        in_specs=(
            P("dp", None, "sp"),
            P("dp", None, "sp"),
            P("dp", None, None),
            P("dp", None, None),
            P(),
            P("dp", "sp"),
            P("dp", "sp"),
        ),
        out_specs=(
            P("dp", None, "sp"),
            P("dp", None, None),
            P("dp", None, None),
            P("dp", "sp"),
            P("dp", "sp"),
        ),
        check_vma=False,
    )
```

```python
import functools

import jax
import jax.numpy as jnp
import numpy as np
from jax import lax
from jax.experimental import pallas as pl
from jax.experimental.pallas import tpu as pltpu
from jax.sharding import PartitionSpec as P

NOPE_DIM = 128
ROPE_DIM = 64
VALUE_DIM = 128
QK = NOPE_DIM + ROPE_DIM
LOG2E = 1.4426950408889634

norm_eps = 1e-06
rope_theta = 10000.0

NT = (((1,), (1,)), ((), ()))
MESH = pl.DeviceIdType.MESH


def rope_tables(length):
    half = ROPE_DIM // 2
    frequency = np.float32(rope_theta) ** (-(np.arange(half, dtype=np.float32) * np.float32(2.0 / ROPE_DIM)))
    angles = np.arange(length, dtype=np.float32)[:, None] * frequency.astype(np.float32)[None, :]
    return np.cos(angles).astype(np.float32), np.sin(angles).astype(np.float32)


def dot(a, b):
    return jnp.dot(a, b, preferred_element_type=jnp.float32)


def dot_nt(a, b):
    return lax.dot_general(a, b, NT, preferred_element_type=jnp.float32)


def swap_halves(x):
    lane = lax.broadcasted_iota(jnp.int32, x.shape, 1)
    return jnp.where(lane % ROPE_DIM < ROPE_DIM // 2, pltpu.roll(x, 96, 1), pltpu.roll(x, 32, 1))


def flat(wide):
    count = wide.shape[0] // 8
    return jnp.concatenate([wide[8 * a:8 * a + 8] for a in range(count)], axis=1)


def unflat(rows):
    count = rows.shape[1] // 128
    return jnp.concatenate([rows[:, 128 * a:128 * a + 128] for a in range(count)], axis=0)


def each(first, count, act):
    def body(k, carry):
        act(k)
        return carry
    lax.fori_loop(first, count, body, 0)


def kernel(
    block, grad_scale, n_sp, n_dp,
    latent_hbm, rope_hbm, gain_hbm, cos_hbm, sin_hbm, cos_t_hbm, sin_t_hbm,
    q_hbm, do_hbm, wk_hbm, wv_hbm,
    dq_ref, grad_ref, low_ref,
    lat, rope, gain, cosw, sinw, cost, sint, doin, w, w_t,
    comp, comp_t, krot, krot_t, ku, kt, vals, qu, pt, dst, dkv, acc, rot_acc,
    part, got_in, got_mid, dwbuf, got_near, red, got_far,
    in_sem, w_sem, q_sem, do_sem,
    far_s, far_r, near_s, near_r, a_s, a_r, m_s, m_r, b_s, b_r, c_s, c_r, d_s, d_r,
):
    sp, dp = lax.axis_index("sp"), lax.axis_index("dp")
    chips = n_dp // 2
    chip, core = dp // 2, lax.rem(dp, 2)
    partner = chip * 2 + 1 - core
    pairs, length = doin.shape[0], doin.shape[1]
    width = lat.shape[1]
    tiles = length // block
    pieces = part.shape[1]
    rows_of = block // pieces
    scale = QK ** (-0.5)
    barrier = pltpu.get_barrier_semaphore()

    def chip_at(k):
        return lax.rem(chip + k, chips)

    def other(k):
        return chip_at(k) * 2 + core

    def source(k):
        return lax.rem(chip - k + chips, chips) * 2 + core

    def w_load(p, t):
        hbm = (wk_hbm, wv_hbm)[t]
        return pltpu.make_async_copy(
            hbm.at[:, pl.ds(pl.multiple_of(p * 256, 256), 256)],
            w.at[p, dp, :, pl.ds(t * 256, 256)], w_sem.at[p, t])

    for t in range(2):
        each(0, pairs, lambda p: w_load(p, t).start())
    each(1, chips, lambda k: pl.semaphore_signal(
        barrier, inc=1, device_id={"dp": other(k)}, device_id_type=MESH))
    lower = sp < n_sp // 2
    at_end = jnp.logical_or(sp == 0, sp == n_sp - 1)
    at_middle = jnp.logical_or(sp == n_sp // 2 - 1, sp == n_sp // 2)
    inward = jnp.where(lower, sp + 1, sp - 1)
    outward = jnp.where(lower, sp - 1, sp + 1)
    pl.semaphore_signal(barrier, inc=1, device_id={"sp": inward}, device_id_type=MESH)
    pl.when(jnp.logical_not(at_end))(lambda: pl.semaphore_signal(
        barrier, inc=1, device_id={"sp": outward}, device_id_type=MESH))
    pl.semaphore_signal(barrier, inc=1, device_id={"dp": partner}, device_id_type=MESH)

    loads = [
        pltpu.make_async_copy(src, dst_, in_sem.at[j]) for j, (src, dst_) in enumerate((
            (latent_hbm, lat), (gain_hbm, gain), (rope_hbm, rope), (cos_t_hbm, cost), (sin_t_hbm, sint),
            (cos_hbm, cosw), (sin_hbm, sinw)))]

    def q_load(p):
        cols = pl.ds(pl.multiple_of(p * 2 * QK, 128), 2 * QK)
        return pltpu.make_async_copy(q_hbm.at[:, cols], dq_ref.at[:, cols], q_sem.at[p])

    def do_load(p):
        return pltpu.make_async_copy(
            do_hbm.at[:, pl.ds(pl.multiple_of(p * 256, 256), 256)], doin.at[p], do_sem.at[p])

    for copy in loads:
        copy.start()
    each(0, pairs, lambda p: q_load(p).start())
    each(0, pairs, lambda p: do_load(p).start())

    def far(p, k):
        return pltpu.make_async_remote_copy(
            src_ref=w.at[p, dp], dst_ref=w.at[p, dp],
            send_sem=far_s.at[p, k], recv_sem=far_r.at[p, k],
            device_id={"dp": other(k)}, device_id_type=MESH)

    def near(p, k):
        row = source(k)
        return pltpu.make_async_remote_copy(
            src_ref=w.at[p, row], dst_ref=w.at[p, row],
            send_sem=near_s.at[p, k], recv_sem=near_r.at[p, k],
            device_id={"dp": partner}, device_id_type=MESH)

    for t in range(2):
        each(0, pairs, lambda p: w_load(p, t).wait())
    pl.semaphore_wait(barrier, chips + jnp.where(at_end, 1, 2))

    def send_weights(p):
        each(1, chips, lambda k: far(p, k).start())
        near(p, 0).start()
    each(0, pairs, send_weights)

    def forward(p):
        def go(k):
            far(p, k).wait_recv()
            near(p, k).start()
        each(1, chips, go)

    for copy in loads:
        copy.wait()
    raw = lat[...].astype(jnp.float32)
    inverse = lax.rsqrt(jnp.mean(raw * raw, axis=-1, keepdims=True) + norm_eps)
    normed = raw * inverse * gain[...]
    comp[...] = normed.astype(jnp.bfloat16)
    comp_t[...] = normed.T.astype(jnp.bfloat16)
    ra = rope[:ROPE_DIM // 2, :].astype(jnp.float32)
    rb = rope[ROPE_DIM // 2:, :].astype(jnp.float32)
    turned = jnp.concatenate([ra * cost[...] - rb * sint[...], rb * cost[...] + ra * sint[...]], axis=0)
    krot_t[...] = turned.astype(jnp.bfloat16)
    krot[...] = jnp.concatenate([turned, turned], axis=0).T.astype(jnp.bfloat16)

    def turn_queries(p):
        q_load(p).wait()
        third = lambda n: dq_ref[:, pl.ds(pl.multiple_of(p * 2 * QK + n * 128, 128), 128)]
        mid = third(1).astype(jnp.float32)
        last = third(2).astype(jnp.float32)
        low = lax.broadcasted_iota(jnp.int32, mid.shape, 1) < 64
        plain = jnp.where(low, pltpu.roll(mid, 64, 1), pltpu.roll(last, 64, 1))
        both = jnp.where(low, mid, last)
        rot = both * cosw[...] + swap_halves(both) * sinw[...]
        qu[2 * p, :, :NOPE_DIM] = third(0)
        qu[2 * p, :, NOPE_DIM:] = rot[:, :ROPE_DIM].astype(jnp.bfloat16)
        qu[2 * p + 1, :, :NOPE_DIM] = plain.astype(jnp.bfloat16)
        qu[2 * p + 1, :, NOPE_DIM:] = pltpu.roll(rot, 64, 1)[:, :ROPE_DIM].astype(jnp.bfloat16)
    each(0, pairs, turn_queries)
    each(0, pairs, lambda p: do_load(p).wait())

    def project(p):
        each(0, chips, lambda k: near(p, k).wait_recv())
        both = dot(comp[...], w[p].reshape(width, 512))
        keys = both[:, :256]
        keys_t = keys.T.astype(jnp.bfloat16)
        keys = keys.astype(jnp.bfloat16)
        vals[p] = both[:, 256:].astype(jnp.bfloat16)
        for h in range(2):
            ku[2 * p + h, :, :NOPE_DIM] = keys[:, h * NOPE_DIM:(h + 1) * NOPE_DIM]
            ku[2 * p + h, :, NOPE_DIM:] = krot[:, :ROPE_DIM]
            kt[2 * p + h, :NOPE_DIM, :] = keys_t[h * NOPE_DIM:(h + 1) * NOPE_DIM, :]
            kt[2 * p + h, NOPE_DIM:, :] = krot_t[...]

    def attend(i, p, h):
        rows = slice(i * block, (i + 1) * block)
        n = (i + 1) * block
        cols = slice(h * VALUE_DIM, (h + 1) * VALUE_DIM)
        scores = dot_nt(ku[2 * p + h, :n, :], qu[2 * p + h, rows, :])
        key_at = lax.broadcasted_iota(jnp.int32, (block, block), 0)
        query_at = lax.broadcasted_iota(jnp.int32, (block, block), 1)
        diag = jnp.where(key_at <= query_at, scores[n - block:], -jnp.inf)
        scores = diag if i == 0 else jnp.concatenate([scores[:n - block], diag], axis=0)
        top = jnp.max(scores, axis=0, keepdims=True)
        e = jnp.exp2((scores - top) * (scale * LOG2E))
        r = 1.0 / jnp.sum(e, axis=0, keepdims=True)
        prob_grad = dot_nt(vals[p, :n, cols], doin[p, rows, cols])
        center = jnp.sum(e * prob_grad, axis=0, keepdims=True) * r
        prob = (e * r).astype(jnp.bfloat16)
        grad = (e * (r * scale) * (prob_grad - center)).astype(jnp.bfloat16)
        for j in range(i + 1):
            at = slice((i - j) * block, (i - j + 1) * block)
            pt[j][2 * p + h, :, at] = prob[j * block:(j + 1) * block]
            dst[j][2 * p + h, :, at] = grad[j * block:(j + 1) * block]

    def key_block(i, p):
        rows = slice(i * block, (i + 1) * block)
        rot = None
        for h in range(2):
            cols = slice(h * VALUE_DIM, (h + 1) * VALUE_DIM)
            dv = dot(pt[i][2 * p + h], doin[p, i * block:, cols])
            dk = dot(dst[i][2 * p + h], qu[2 * p + h, i * block:, :])
            dkv[p, rows, h * NOPE_DIM:(h + 1) * NOPE_DIM] = dk[:, :NOPE_DIM].astype(jnp.bfloat16)
            dkv[p, rows, (2 + h) * 128:(3 + h) * 128] = dv.astype(jnp.bfloat16)
            rot = dk[:, NOPE_DIM:] if rot is None else rot + dk[:, NOPE_DIM:]
        rot_acc[...] += rot
        acc[...] += dot(dkv[p, rows, :], w_t[p])

    def in_copy(i, q):
        return pltpu.make_async_remote_copy(
            src_ref=part.at[i, q], dst_ref=got_in.at[i, q],
            send_sem=a_s.at[i, q], recv_sem=a_r.at[i, q],
            device_id={"sp": inward}, device_id_type=MESH)

    def mid_copy(i, q):
        return pltpu.make_async_remote_copy(
            src_ref=part.at[i, q], dst_ref=got_mid.at[i, q],
            send_sem=m_s.at[i, q], recv_sem=m_r.at[i, q],
            device_id={"sp": inward}, device_id_type=MESH)

    def out_copy(i, q):
        return pltpu.make_async_remote_copy(
            src_ref=low_ref.at[i, q], dst_ref=low_ref.at[i, q],
            send_sem=b_s.at[i, q], recv_sem=b_r.at[i, q],
            device_id={"sp": outward}, device_id_type=MESH)

    def go_in(i, q):
        pl.when(at_middle)(lambda: mid_copy(i, q).start())
        pl.when(jnp.logical_not(at_middle))(lambda: in_copy(i, q).start())

    def send_part(i):
        for q in range(pieces):
            mine = slice(q * rows_of, (q + 1) * rows_of)
            part[i, q, :rows_of] = acc[mine].astype(jnp.bfloat16)
            rot = rot_acc[mine]
            wide = jnp.concatenate([rot[:rows_of // 2], rot[rows_of // 2:]], axis=1)
            part[i, q, rows_of:] = flat(wide).astype(jnp.bfloat16)
        def go():
            for q in range(pieces):
                go_in(i, q)
        pl.when(at_end)(go)

    def merge(i, q):
        def go():
            in_copy(i, q).wait_recv()
            part[i, q] = (part[i, q].astype(jnp.float32) + got_in[i, q].astype(jnp.float32)).astype(jnp.bfloat16)
            go_in(i, q)
        pl.when(jnp.logical_not(at_end))(go)

    def finish(i, q):
        def go():
            mid_copy(i, q).wait_recv()
            total = part[i, q].astype(jnp.float32) + got_mid[i, q].astype(jnp.float32)
            mine = slice(i * block + q * rows_of, i * block + (q + 1) * rows_of)
            raw = lat[mine, :].astype(jnp.float32)
            inverse = lax.rsqrt(jnp.mean(raw * raw, axis=-1, keepdims=True) + norm_eps)
            mixed = total[:rows_of] * gain[...]
            spread = jnp.mean(raw * mixed, axis=-1, keepdims=True)
            low_ref[i, q, :rows_of] = (inverse * mixed - raw * inverse**3 * spread).astype(jnp.bfloat16)
            rot = unflat(total[rows_of:])
            left = lax.broadcasted_iota(jnp.int32, rot.shape, 1) < ROPE_DIM
            c, s = (jnp.where(left, t[:rows_of // 2], t[rows_of // 2:]) for t in (cosw[mine, :], sinw[mine, :]))
            low_ref[i, q, rows_of:] = flat(rot * c - swap_halves(rot) * s).astype(jnp.bfloat16)
            pl.when(jnp.logical_not(at_end))(lambda: out_copy(i, q).start())
        pl.when(at_middle)(go)

    def deliver(i, q):
        def go():
            out_copy(i, q).wait_recv()
            pl.when(jnp.logical_not(at_end))(lambda: out_copy(i, q).start())
        pl.when(jnp.logical_not(at_middle))(go)

    def drain_rows(i, q):
        pl.when(at_middle)(lambda: mid_copy(i, q).wait_send())
        pl.when(jnp.logical_not(at_middle))(lambda: in_copy(i, q).wait_send())
        pl.when(jnp.logical_not(at_end))(lambda: out_copy(i, q).wait_send())

    def near_grad(p):
        return pltpu.make_async_remote_copy(
            src_ref=dwbuf.at[p, 1 - core], dst_ref=got_near.at[p],
            send_sem=c_s.at[p], recv_sem=c_r.at[p],
            device_id={"dp": partner}, device_id_type=MESH)

    def far_grad(p, k):
        return pltpu.make_async_remote_copy(
            src_ref=red.at[p, chip_at(k)], dst_ref=got_far.at[p, k],
            send_sem=d_s.at[p, k], recv_sem=d_r.at[p, k],
            device_id={"dp": other(k)}, device_id_type=MESH)

    def weight_grad(p):
        dw = dot(comp_t[...], dkv[p]) * grad_scale
        dw = dw.reshape(chips, 2, width // n_dp, 512)
        for c in range(2):
            dwbuf[p, c] = dw[:, c].astype(jnp.bfloat16)
        near_grad(p).start()

    def chip_grad(p):
        near_grad(p).wait_recv()
        both = dwbuf[p, core].astype(jnp.float32) + got_near[p].astype(jnp.float32)
        red[p] = both.astype(jnp.bfloat16)
        each(1, chips, lambda k: far_grad(p, k).start())

    def query_grad(i, p):
        rows = slice(i * block, (i + 1) * block)
        n = (i + 1) * block
        parts = []
        for h in range(2):
            g = dot(kt[2 * p + h, :, :n], jnp.concatenate(
                [dst[j][2 * p + h, :, (i - j) * block:(i - j + 1) * block] for j in range(i + 1)], axis=0))
            a = g[NOPE_DIM:NOPE_DIM + 32]
            b = g[NOPE_DIM + 32:]
            c, s = cost[:, rows], sint[:, rows]
            parts += [g[:NOPE_DIM], a * c + b * s, b * c - a * s]
        dq_ref[rows, pl.ds(pl.multiple_of(p * 2 * QK, 128), 2 * QK)] = (
            jnp.concatenate(parts, axis=0).T.astype(jnp.bfloat16))

    last = pairs - 1
    stages = {}

    def stage(act, i, *keys):
        for q, key in enumerate(keys):
            phase, at = key if isinstance(key, tuple) else (key, None)
            key = phase if at is None else (phase, min(at, last))
            stages.setdefault(key, []).append(functools.partial(act, i, q))

    for i in range(tiles - 1, 0, -1):
        if i > 1:
            stage(merge, i, (i - 1, 2), (i - 1, 3), ("sent", i - 1), (i - 2, 0))
            stage(finish, i, (i - 2, 1), (i - 2, 2), (i - 2, 3), ("w", 0))
        else:
            stage(merge, 1, (0, 2), (0, 3), ("w", 0), ("w", 2))
            stage(finish, 1, ("w", 3), "grads", ("q2", 1), ("q2", 3))
    stage(merge, 0, ("q2", 1), ("q2", 3), ("q1", 1), ("q1", 3))
    stage(finish, 0, ("q0", 0), ("q0", 3), "end", "end")

    def run(key):
        for act in stages.pop(key, []):
            act()

    def run_in(name, p):
        for at in range(pairs):
            if (name, at) in stages:
                pl.when(p == at)(functools.partial(run, (name, at)))

    forward(0)
    for i in reversed(range(tiles)):
        acc[...] = jnp.zeros_like(acc)
        rot_acc[...] = jnp.zeros_like(rot_acc)

        def step(p, i=i):
            if i == tiles - 1:
                project(p)
            attend(i, p, 0)
            if i == tiles - 1:
                pl.when(p + 1 < pairs)(lambda: forward(p + 1))
                w_t[p] = w[p].reshape(width, 512).T
            attend(i, p, 1)
            key_block(i, p)
            run_in(i, p)
        each(0, pairs, step)
        send_part(i)
        run(("sent", min(i, last)))

    def grads(p):
        weight_grad(p)
        pl.when(p > 1)(lambda: chip_grad(p - 2))
        run_in("w", p)
    each(0, pairs, grads)
    for p in range(max(pairs - 2, 0), pairs):
        chip_grad(p)
    run("grads")

    for i in reversed(range(tiles)):
        def turn_back(p, i=i):
            query_grad(i, p)
            run_in("q" + str(i), p)
        each(0, pairs, turn_back)
    for key in sorted(k for k in stages if isinstance(k, str)):
        run(key)
    assert not stages

    def add(p):
        total = red[p, chip].astype(jnp.float32)
        for k in range(1, chips):
            far_grad(p, k).wait()
            total = total + got_far[p, k].astype(jnp.float32)
        cols = pl.ds(pl.multiple_of(p * 256, 256), 256)
        grad_ref[0, :, cols] = total[:, :256]
        grad_ref[1, :, cols] = total[:, 256:]
        near_grad(p).wait_send()
        def drain(k):
            far(p, k).wait_send()
            near(p, k).wait_send()
        each(1, chips, drain)
        near(p, 0).wait_send()
    each(0, pairs, add)
    for i in reversed(range(tiles)):
        for q in range(pieces):
            deliver(i, q)
            drain_rows(i, q)


def fused(queries, out_grad, latent, rope_t, kv_gain, key_up, value_up, grad_scale, n_sp, n_dp):
    length, width = latent.shape
    pairs = key_up.shape[1] // 256
    heads = 2 * pairs
    chips = n_dp // 2
    block = 256
    tiles = length // block
    pieces = 4
    rows = block // pieces
    piece = (tiles, pieces, rows + rows * ROPE_DIM // width, width)
    depth = key_up.shape[0]
    cosine, sine = rope_tables(length)
    bf, f32 = jnp.bfloat16, jnp.float32
    hbm = pl.BlockSpec(memory_space=pltpu.HBM)
    vmem = pl.BlockSpec(memory_space=pltpu.VMEM)
    dma = lambda *n: pltpu.SemaphoreType.DMA(n)
    V = pltpu.VMEM
    triangle = tuple(V((heads, block, length - j * block), bf) for j in range(tiles))
    return pl.pallas_call(
        functools.partial(kernel, block, grad_scale, n_sp, n_dp),
        in_specs=[hbm] * 11,
        out_specs=[vmem] * 3,
        out_shape=[
            jax.ShapeDtypeStruct(queries.shape, bf),
            jax.ShapeDtypeStruct((2, *key_up.shape), f32),
            jax.ShapeDtypeStruct(piece, bf),
        ],
        scratch_shapes=[
            V((length, width), bf), V((ROPE_DIM, length), bf), V((1, width), f32),
            V((length, 128), f32), V((length, 128), f32), V((32, length), f32), V((32, length), f32),
            V((pairs, length, 256), bf), V((pairs, n_dp, depth, 512), bf), V((pairs, 512, width), bf),
            V((length, width), bf), V((width, length), bf), V((length, 128), bf), V((ROPE_DIM, length), bf),
            V((heads, length, QK), bf), V((heads, QK, length), bf), V((pairs, length, 256), bf),
            V((heads, length, QK), bf), triangle, triangle,
            V((pairs, length, 512), bf), V((block, width), f32), V((block, ROPE_DIM), f32),
            V(piece, bf), V(piece, bf), V(piece, bf),
            V((pairs, 2, chips, depth, 512), bf), V((pairs, chips, depth, 512), bf),
            V((pairs, chips, depth, 512), bf), V((pairs, chips, depth, 512), bf),
            dma(7), dma(pairs, 2), dma(pairs), dma(pairs),
            dma(pairs, chips), dma(pairs, chips), dma(pairs, chips), dma(pairs, chips),
            *[dma(tiles, pieces)] * 6,
            dma(pairs), dma(pairs), dma(pairs, chips), dma(pairs, chips),
        ],
        compiler_params=pltpu.CompilerParams(
            collective_id=0, has_side_effects=True, vmem_limit_bytes=50 * 1024 * 1024
        ),
        name="fused_backward",
    )(*(pltpu.with_memory_space_constraint(jnp.asarray(x), pltpu.HBM) for x in (
        latent, rope_t, kv_gain.reshape(1, -1), np.tile(cosine, (1, 4)),
        np.concatenate([-sine, sine, -sine, sine], axis=1),
        np.ascontiguousarray(cosine.T), np.ascontiguousarray(sine.T),
        queries, out_grad, key_up, value_up,
    )))


def write_kernel(dq_ref, grad_ref, low_ref, dq_out, lat_out, rot_out, key_out, value_out, rot, sem):
    count, rows = low_ref.shape[0], lat_out.shape[0] // low_ref.shape[0]
    copies = [
        pltpu.make_async_copy(src, dst_, sem.at[j]) for j, (src, dst_) in enumerate((
            (dq_ref, dq_out), (grad_ref.at[0], key_out), (grad_ref.at[1], value_out), (rot, rot_out)))]
    copies += [
        pltpu.make_async_copy(
            low_ref.at[j, pl.ds(0, rows)], lat_out.at[pl.ds(j * rows, rows)], sem.at[4 + j])
        for j in range(count)]
    for j, copy in enumerate(copies):
        if j != 3:
            copy.start()
    turned = []
    for j in range(count):
        wide = unflat(low_ref[j, rows:].astype(jnp.float32))
        turned += [wide, pltpu.roll(wide, 64, 1)]
    rot[...] = jnp.concatenate(turned, axis=0).T[:ROPE_DIM].astype(jnp.bfloat16)
    copies[3].start()
    for copy in copies:
        copy.wait()


def write(dq, grad, low, length):
    width = low.shape[2]
    bf, f32 = jnp.bfloat16, jnp.float32
    return pl.pallas_call(
        write_kernel,
        in_specs=[pl.BlockSpec(memory_space=pltpu.VMEM)] * 3,
        out_specs=[pl.BlockSpec(memory_space=pl.ANY)] * 5,
        out_shape=[
            jax.ShapeDtypeStruct(dq.shape, bf),
            jax.ShapeDtypeStruct((length, width), bf),
            jax.ShapeDtypeStruct((ROPE_DIM, length), bf),
            jax.ShapeDtypeStruct(grad.shape[1:], f32),
            jax.ShapeDtypeStruct(grad.shape[1:], f32),
        ],
        scratch_shapes=[pltpu.VMEM((ROPE_DIM, length), bf), pltpu.SemaphoreType.DMA((4 + low.shape[0],))],
        compiler_params=pltpu.CompilerParams(vmem_limit_bytes=16 * 1024 * 1024),
        name="write_outputs",
    )(dq, grad, low)


def shards(queries, out_grad, latent, rope_key, kv_gain, key_up, value_up):
    length, width = latent.shape[1:]
    n_sp, n_dp = lax.axis_size("sp"), lax.axis_size("dp")
    grad_scale = float(n_dp * length) ** (-0.5)
    rope_t = jnp.swapaxes(rope_key, 1, 2)[0]
    dq, grad, low = fused(
        queries[0], out_grad[0], latent[0], rope_t, kv_gain, key_up, value_up, grad_scale, n_sp, n_dp
    )
    dq, lat, rot_t, key_grad, value_grad = write(dq, grad, low.reshape(-1, *low.shape[2:]), length)
    return dq[None], lat[None], jnp.swapaxes(rot_t[None], 1, 2), key_grad, value_grad


def solution(mesh):
    return jax.shard_map(
        shards,
        mesh=mesh,
        in_specs=(
            P("dp", None, "sp"),
            P("dp", None, "sp"),
            P("dp", None, None),
            P("dp", None, None),
            P(),
            P("dp", "sp"),
            P("dp", "sp"),
        ),
        out_specs=(
            P("dp", None, "sp"),
            P("dp", None, None),
            P("dp", None, None),
            P("dp", "sp"),
            P("dp", "sp"),
        ),
        check_vma=False,
    )
```

```python
import functools

import jax
import jax.numpy as jnp
import numpy as np
from jax import lax
from jax.experimental import pallas as pl
from jax.experimental.pallas import tpu as pltpu
from jax.sharding import PartitionSpec as P

NOPE_DIM = 128
ROPE_DIM = 64
VALUE_DIM = 128
QK = NOPE_DIM + ROPE_DIM
LOG2E = 1.4426950408889634

norm_eps = 1e-06
rope_theta = 10000.0

NT = (((1,), (1,)), ((), ()))
MESH = pl.DeviceIdType.MESH


def rope_tables(length):
    half = ROPE_DIM // 2
    frequency = np.float32(rope_theta) ** (-(np.arange(half, dtype=np.float32) * np.float32(2.0 / ROPE_DIM)))
    angles = np.arange(length, dtype=np.float32)[:, None] * frequency.astype(np.float32)[None, :]
    return np.cos(angles).astype(np.float32), np.sin(angles).astype(np.float32)


def dot(a, b):
    return jnp.dot(a, b, preferred_element_type=jnp.float32)


def dot_nt(a, b):
    return lax.dot_general(a, b, NT, preferred_element_type=jnp.float32)


def swap_halves(x):
    lane = lax.broadcasted_iota(jnp.int32, x.shape, 1)
    return jnp.where(lane % ROPE_DIM < ROPE_DIM // 2, pltpu.roll(x, 96, 1), pltpu.roll(x, 32, 1))


def flat(wide):
    count = wide.shape[0] // 8
    return jnp.concatenate([wide[8 * a:8 * a + 8] for a in range(count)], axis=1)


def unflat(rows):
    count = rows.shape[1] // 128
    return jnp.concatenate([rows[:, 128 * a:128 * a + 128] for a in range(count)], axis=0)


def each(first, count, act):
    def body(k, carry):
        act(k)
        return carry
    lax.fori_loop(first, count, body, 0)


def kernel(
    block, grad_scale, n_sp, n_dp,
    latent_hbm, rope_hbm, gain_hbm, cos_hbm, sin_hbm, cos_t_hbm, sin_t_hbm,
    q_hbm, do_hbm, wk_hbm, wv_hbm,
    dq_ref, grad_ref, low_ref,
    lat, rope, gain, cosw, sinw, cost, sint, doin, w,
    comp, comp_t, krot, krot_t, ku, kt, vals, qu, pt, dst, dkv, acc, rot_acc,
    part, got_in, got_mid, dwbuf, got_near, red, got_far,
    in_sem, w_sem, do_sem,
    far_s, far_r, near_s, near_r, a_s, a_r, b_s, b_r, c_s, c_r, d_s, d_r,
):
    sp, dp = lax.axis_index("sp"), lax.axis_index("dp")
    chips = n_dp // 2
    chip, core = dp // 2, lax.rem(dp, 2)
    partner = chip * 2 + 1 - core
    pairs, length = doin.shape[0], doin.shape[1]
    width = lat.shape[1]
    tiles = length // block
    pieces = part.shape[1]
    rows_of = block // pieces
    scale = QK ** (-0.5)
    barrier = pltpu.get_barrier_semaphore()

    def chip_at(k):
        return lax.rem(chip + k, chips)

    def other(k):
        return chip_at(k) * 2 + core

    def source(k):
        return lax.rem(chip - k + chips, chips) * 2 + core

    def w_load(p, t):
        hbm = (wk_hbm, wv_hbm)[t]
        return pltpu.make_async_copy(
            hbm.at[:, pl.ds(pl.multiple_of(p * 256, 256), 256)],
            w.at[p, dp, :, pl.ds(t * 256, 256)], w_sem.at[0])

    for t in range(2):
        each(0, pairs, lambda p: w_load(p, t).start())
    each(1, chips, lambda k: pl.semaphore_signal(
        barrier, inc=1, device_id={"dp": other(k)}, device_id_type=MESH))
    lower = sp < n_sp // 2
    at_end = jnp.logical_or(sp == 0, sp == n_sp - 1)
    at_middle = jnp.logical_or(sp == n_sp // 2 - 1, sp == n_sp // 2)
    inward = jnp.where(lower, sp + 1, sp - 1)
    outward = jnp.where(lower, sp - 1, sp + 1)
    pl.semaphore_signal(barrier, inc=1, device_id={"sp": inward}, device_id_type=MESH)
    pl.when(jnp.logical_not(at_end))(lambda: pl.semaphore_signal(
        barrier, inc=1, device_id={"sp": outward}, device_id_type=MESH))
    pl.semaphore_signal(barrier, inc=1, device_id={"dp": partner}, device_id_type=MESH)

    loads = [
        pltpu.make_async_copy(src, dst_, in_sem.at[j]) for j, (src, dst_) in enumerate((
            (q_hbm, dq_ref), (latent_hbm, lat), (gain_hbm, gain), (rope_hbm, rope), (cos_t_hbm, cost), (sin_t_hbm, sint),
            (cos_hbm, cosw), (sin_hbm, sinw)))]

    def do_load(p):
        return pltpu.make_async_copy(
            do_hbm.at[:, pl.ds(pl.multiple_of(p * 256, 256), 256)], doin.at[p], do_sem.at[0])

    for copy in loads:
        copy.start()
    each(0, pairs, lambda p: do_load(p).start())

    def far(p, k):
        return pltpu.make_async_remote_copy(
            src_ref=w.at[p, dp], dst_ref=w.at[p, dp],
            send_sem=far_s.at[0], recv_sem=far_r.at[p],
            device_id={"dp": other(k)}, device_id_type=MESH)

    def near(p, k):
        row = source(k)
        return pltpu.make_async_remote_copy(
            src_ref=w.at[p, row], dst_ref=w.at[p, row],
            send_sem=near_s.at[0], recv_sem=near_r.at[p],
            device_id={"dp": partner}, device_id_type=MESH)

    pltpu.make_async_copy(w.at[:, dp], w.at[:, dp], w_sem.at[0]).wait()
    pl.semaphore_wait(barrier, chips + jnp.where(at_end, 1, 2))

    def send_weights(p):
        each(1, chips, lambda k: far(p, k).start())
        near(p, 0).start()
    each(0, pairs, send_weights)

    def blocks_in(ref, sem):
        return pltpu.make_async_copy(ref, ref, sem)

    def forward(p):
        blocks_in(w.at[p, pl.ds(0, chips - 1)], far_r.at[p]).wait()
        each(1, chips, lambda k: near(p, k).start())

    for copy in loads:
        copy.wait()
    raw = lat[...].astype(jnp.float32)
    inverse = lax.rsqrt(jnp.mean(raw * raw, axis=-1, keepdims=True) + norm_eps)
    normed = raw * inverse * gain[...]
    comp[...] = normed.astype(jnp.bfloat16)
    comp_t[...] = normed.T.astype(jnp.bfloat16)
    ra = rope[:ROPE_DIM // 2, :].astype(jnp.float32)
    rb = rope[ROPE_DIM // 2:, :].astype(jnp.float32)
    turned = jnp.concatenate([ra * cost[...] - rb * sint[...], rb * cost[...] + ra * sint[...]], axis=0)
    krot_t[...] = turned.astype(jnp.bfloat16)
    krot[...] = jnp.concatenate([turned, turned], axis=0).T.astype(jnp.bfloat16)

    def turn_queries(p):
        third = lambda n: dq_ref[:, pl.ds(pl.multiple_of(p * 2 * QK + n * 128, 128), 128)]
        mid = third(1).astype(jnp.float32)
        last = third(2).astype(jnp.float32)
        low = lax.broadcasted_iota(jnp.int32, mid.shape, 1) < 64
        plain = jnp.where(low, pltpu.roll(mid, 64, 1), pltpu.roll(last, 64, 1))
        both = jnp.where(low, mid, last)
        rot = both * cosw[...] + swap_halves(both) * sinw[...]
        qu[2 * p, :, :NOPE_DIM] = third(0)
        qu[2 * p, :, NOPE_DIM:] = rot[:, :ROPE_DIM].astype(jnp.bfloat16)
        qu[2 * p + 1, :, :NOPE_DIM] = plain.astype(jnp.bfloat16)
        qu[2 * p + 1, :, NOPE_DIM:] = pltpu.roll(rot, 64, 1)[:, :ROPE_DIM].astype(jnp.bfloat16)
    each(0, pairs, turn_queries)
    pltpu.make_async_copy(doin, doin, do_sem.at[0]).wait()

    def project(p):
        blocks_in(w.at[p, pl.ds(0, chips)], near_r.at[p]).wait()
        both = dot(comp[...], w[p].reshape(width, 512))
        keys = both[:, :256]
        keys = keys.astype(jnp.bfloat16)
        vals[p] = both[:, 256:].astype(jnp.bfloat16)
        for h in range(2):
            ku[2 * p + h, :, :NOPE_DIM] = keys[:, h * NOPE_DIM:(h + 1) * NOPE_DIM]
            ku[2 * p + h, :, NOPE_DIM:] = krot[:, :ROPE_DIM]

    def attend(i, p, h):
        rows = slice(i * block, (i + 1) * block)
        n = (i + 1) * block
        cols = slice(h * VALUE_DIM, (h + 1) * VALUE_DIM)
        scores = dot_nt(ku[2 * p + h, :n, :], qu[2 * p + h, rows, :])
        key_at = lax.broadcasted_iota(jnp.int32, (block, block), 0)
        query_at = lax.broadcasted_iota(jnp.int32, (block, block), 1)
        diag = jnp.where(key_at <= query_at, scores[n - block:], -jnp.inf)
        scores = diag if i == 0 else jnp.concatenate([scores[:n - block], diag], axis=0)
        top = jnp.max(scores, axis=0, keepdims=True)
        e = jnp.exp2((scores - top) * (scale * LOG2E))
        r = 1.0 / jnp.sum(e, axis=0, keepdims=True)
        prob_grad = dot_nt(vals[p, :n, cols], doin[p, rows, cols])
        center = jnp.sum(e * prob_grad, axis=0, keepdims=True) * r
        prob = (e * r).astype(jnp.bfloat16)
        grad = (e * (r * scale) * (prob_grad - center)).astype(jnp.bfloat16)
        for j in range(i + 1):
            at = slice((i - j) * block, (i - j + 1) * block)
            pt[j][2 * p + h, :, at] = prob[j * block:(j + 1) * block]
            dst[j][2 * p + h, :, at] = grad[j * block:(j + 1) * block]

    def key_block(i, p):
        rows = slice(i * block, (i + 1) * block)
        rot = None
        for h in range(2):
            cols = slice(h * VALUE_DIM, (h + 1) * VALUE_DIM)
            dv = dot(pt[i][2 * p + h], doin[p, i * block:, cols])
            dk = dot(dst[i][2 * p + h], qu[2 * p + h, i * block:, :])
            dkv[p, rows, h * NOPE_DIM:(h + 1) * NOPE_DIM] = dk[:, :NOPE_DIM].astype(jnp.bfloat16)
            dkv[p, rows, (2 + h) * 128:(3 + h) * 128] = dv.astype(jnp.bfloat16)
            rot = dk[:, NOPE_DIM:] if rot is None else rot + dk[:, NOPE_DIM:]
        rot_acc[...] += rot

    def in_copy(i, q):
        return pltpu.make_async_remote_copy(
            src_ref=part.at[i, q], dst_ref=got_in.at[i, q],
            send_sem=a_s.at[0], recv_sem=a_r.at[i, q],
            device_id={"sp": inward}, device_id_type=MESH)

    def mid_copy(i, q):
        return pltpu.make_async_remote_copy(
            src_ref=part.at[i, q], dst_ref=got_mid.at[i, q],
            send_sem=a_s.at[0], recv_sem=b_r.at[i, q],
            device_id={"sp": inward}, device_id_type=MESH)

    def out_copy(i, q):
        return pltpu.make_async_remote_copy(
            src_ref=low_ref.at[i, q], dst_ref=low_ref.at[i, q],
            send_sem=b_s.at[0], recv_sem=b_r.at[i, q],
            device_id={"sp": outward}, device_id_type=MESH)

    def go_in(i, q):
        pl.when(at_middle)(lambda: mid_copy(i, q).start())
        pl.when(jnp.logical_not(at_middle))(lambda: in_copy(i, q).start())

    def send_part(i):
        total = None
        for p in range(pairs):
            term = dot_nt(dkv[p, i * block:(i + 1) * block, :], w[p].reshape(width, 512))
            total = term if total is None else total + term
        acc[...] = total
        for q in range(pieces):
            mine = slice(q * rows_of, (q + 1) * rows_of)
            part[i, q, :rows_of] = acc[mine].astype(jnp.bfloat16)
            rot = rot_acc[mine]
            wide = jnp.concatenate([rot[:rows_of // 2], rot[rows_of // 2:]], axis=1)
            part[i, q, rows_of:] = flat(wide).astype(jnp.bfloat16)
        def go():
            for q in range(pieces):
                go_in(i, q)
        pl.when(at_end)(go)

    def merge(i, q):
        def go():
            in_copy(i, q).wait_recv()
            part[i, q] = (part[i, q].astype(jnp.float32) + got_in[i, q].astype(jnp.float32)).astype(jnp.bfloat16)
            go_in(i, q)
        pl.when(jnp.logical_not(at_end))(go)

    def finish(i, q):
        def go():
            mid_copy(i, q).wait_recv()
            total = part[i, q].astype(jnp.float32) + got_mid[i, q].astype(jnp.float32)
            mine = slice(i * block + q * rows_of, i * block + (q + 1) * rows_of)
            raw = lat[mine, :].astype(jnp.float32)
            inverse = lax.rsqrt(jnp.mean(raw * raw, axis=-1, keepdims=True) + norm_eps)
            mixed = total[:rows_of] * gain[...]
            spread = jnp.mean(raw * mixed, axis=-1, keepdims=True)
            low_ref[i, q, :rows_of] = (inverse * mixed - raw * inverse**3 * spread).astype(jnp.bfloat16)
            rot = unflat(total[rows_of:])
            left = lax.broadcasted_iota(jnp.int32, rot.shape, 1) < ROPE_DIM
            c, s = (jnp.where(left, t[:rows_of // 2], t[rows_of // 2:]) for t in (cosw[mine, :], sinw[mine, :]))
            low_ref[i, q, rows_of:] = flat(rot * c - swap_halves(rot) * s).astype(jnp.bfloat16)
            pl.when(jnp.logical_not(at_end))(lambda: out_copy(i, q).start())
        pl.when(at_middle)(go)

    def deliver(i, q):
        def go():
            out_copy(i, q).wait_recv()
            pl.when(jnp.logical_not(at_end))(lambda: out_copy(i, q).start())
        pl.when(jnp.logical_not(at_middle))(go)

    def near_grad(p):
        return pltpu.make_async_remote_copy(
            src_ref=dwbuf.at[p, 1 - core], dst_ref=got_near.at[p],
            send_sem=c_s.at[0], recv_sem=c_r.at[p],
            device_id={"dp": partner}, device_id_type=MESH)

    def far_grad(p, k):
        return pltpu.make_async_remote_copy(
            src_ref=red.at[p, chip_at(k)], dst_ref=got_far.at[p, k],
            send_sem=d_s.at[0], recv_sem=d_r.at[p],
            device_id={"dp": other(k)}, device_id_type=MESH)

    def weight_grad(p):
        dw = dot(comp_t[...], dkv[p]) * grad_scale
        dw = dw.reshape(chips, 2, width // n_dp, 512)
        for c in range(2):
            dwbuf[p, c] = dw[:, c].astype(jnp.bfloat16)
        near_grad(p).start()

    def chip_grad(p):
        near_grad(p).wait_recv()
        both = dwbuf[p, core].astype(jnp.float32) + got_near[p].astype(jnp.float32)
        red[p] = both.astype(jnp.bfloat16)
        each(1, chips, lambda k: far_grad(p, k).start())

    def query_grad(i, p):
        rows = slice(i * block, (i + 1) * block)
        n = (i + 1) * block
        parts = []
        for h in range(2):
            if i == tiles - 1:
                plain = ku[2 * p + h, :, :NOPE_DIM].astype(jnp.float32)
                kt[2 * p + h, :NOPE_DIM, :] = plain.T.astype(jnp.bfloat16)
                kt[2 * p + h, NOPE_DIM:, :] = krot_t[...]
            g = dot(kt[2 * p + h, :, :n], jnp.concatenate(
                [dst[j][2 * p + h, :, (i - j) * block:(i - j + 1) * block] for j in range(i + 1)], axis=0))
            a = g[NOPE_DIM:NOPE_DIM + 32]
            b = g[NOPE_DIM + 32:]
            c, s = cost[:, rows], sint[:, rows]
            parts += [g[:NOPE_DIM], a * c + b * s, b * c - a * s]
        dq_ref[rows, pl.ds(pl.multiple_of(p * 2 * QK, 128), 2 * QK)] = (
            jnp.concatenate(parts, axis=0).T.astype(jnp.bfloat16))

    last = pairs - 1
    stages = {}

    def stage(act, i, *keys):
        for q, key in enumerate(keys):
            phase, at = key if isinstance(key, tuple) else (key, None)
            key = phase if at is None else (phase, min(at, last))
            stages.setdefault(key, []).append(functools.partial(act, i, q))

    stage(merge, 0, ("w", 1), ("w", 3), ("q2", 0), ("q2", 3))
    for i in range(tiles - 1, 0, -1):
        if i > 1:
            stage(merge, i, (i - 1, 2), (i - 1, 3), ("sent", i - 1), (i - 2, 0))
            stage(finish, i, (i - 2, 0), (i - 2, 1), (i - 2, 2), (i - 2, 3))
        else:
            stage(merge, 1, (0, 1), (0, 2), (0, 3), ("w", 0))
            stage(finish, 1, ("w", 1), ("w", 2), ("w", 3), "grads")
    stage(finish, 0, ("q2", 1), ("q1", 0), ("q0", 0), "end")

    def run(key):
        for act in stages.pop(key, []):
            act()

    def run_in(name, p):
        for at in range(pairs):
            if (name, at) in stages:
                pl.when(p == at)(functools.partial(run, (name, at)))

    forward(0)
    for i in reversed(range(tiles)):
        rot_acc[...] = jnp.zeros_like(rot_acc)

        def step(p, i=i):
            if i == tiles - 1:
                project(p)
                pl.when(jnp.logical_and(p > 0, p < last))(lambda: forward(p + 1))
            attend(i, p, 0)
            attend(i, p, 1)
            if i == tiles - 1 and last > 0:
                pl.when(p == 0)(lambda: forward(1))
            key_block(i, p)
            run_in(i, p)
            if i == 0:
                pl.when(p == last)(lambda: weight_grad(0))
        each(0, pairs, step)
        send_part(i)
        run(("sent", min(i, last)))

    run(("w", 0))

    def grads(p):
        weight_grad(p)
        pl.when(p == 1)(lambda: chip_grad(0))
        pl.when(p > 2)(lambda: chip_grad(p - 2))
        run_in("w", p)
    each(1, pairs, grads)
    for p in range(pairs):
        if p >= pairs - 2 and not (p == 0 and pairs > 1):
            chip_grad(p)
    run("grads")

    for i in reversed(range(tiles)):
        def turn_back(p, i=i):
            query_grad(i, p)
            run_in("q" + str(i), p)
        each(0, pairs, turn_back)
    for key in sorted(k for k in stages if isinstance(k, str)):
        run(key)
    assert not stages

    def add(p):
        blocks_in(got_far.at[p, pl.ds(1, chips - 1)], d_r.at[p]).wait()
        total = red[p, chip].astype(jnp.float32)
        for k in range(1, chips):
            total = total + got_far[p, k].astype(jnp.float32)
        cols = pl.ds(pl.multiple_of(p * 256, 256), 256)
        grad_ref[0, :, cols] = total[:, :256]
        grad_ref[1, :, cols] = total[:, 256:]
    each(0, pairs, add)
    blocks_in(w.at[:, pl.ds(0, chips - 1)], far_s.at[0]).wait()
    blocks_in(w.at[:, pl.ds(0, chips)], near_s.at[0]).wait()
    blocks_in(got_near, c_s.at[0]).wait()
    blocks_in(red.at[:, pl.ds(0, chips - 1)], d_s.at[0]).wait()
    blocks_in(part, a_s.at[0]).wait()
    for i in reversed(range(tiles)):
        for q in range(pieces):
            deliver(i, q)
    pl.when(jnp.logical_not(at_end))(lambda: blocks_in(part, b_s.at[0]).wait())


def fused(queries, out_grad, latent, rope_t, kv_gain, key_up, value_up, grad_scale, n_sp, n_dp):
    length, width = latent.shape
    pairs = key_up.shape[1] // 256
    heads = 2 * pairs
    chips = n_dp // 2
    block = 256
    tiles = length // block
    pieces = 4
    rows = block // pieces
    piece = (tiles, pieces, rows + rows * ROPE_DIM // width, width)
    depth = key_up.shape[0]
    cosine, sine = rope_tables(length)
    bf, f32 = jnp.bfloat16, jnp.float32
    hbm = pl.BlockSpec(memory_space=pltpu.HBM)
    vmem = pl.BlockSpec(memory_space=pltpu.VMEM)
    dma = lambda *n: pltpu.SemaphoreType.DMA(n)
    V = pltpu.VMEM
    triangle = tuple(V((heads, block, length - j * block), bf) for j in range(tiles))
    return pl.pallas_call(
        functools.partial(kernel, block, grad_scale, n_sp, n_dp),
        in_specs=[hbm] * 11,
        out_specs=[vmem] * 3,
        out_shape=[
            jax.ShapeDtypeStruct(queries.shape, bf),
            jax.ShapeDtypeStruct((2, *key_up.shape), f32),
            jax.ShapeDtypeStruct(piece, bf),
        ],
        scratch_shapes=[
            V((length, width), bf), V((ROPE_DIM, length), bf), V((1, width), f32),
            V((length, 128), f32), V((length, 128), f32), V((32, length), f32), V((32, length), f32),
            V((pairs, length, 256), bf), V((pairs, n_dp, depth, 512), bf),
            V((length, width), bf), V((width, length), bf), V((length, 128), bf), V((ROPE_DIM, length), bf),
            V((heads, length, QK), bf), V((heads, QK, length), bf), V((pairs, length, 256), bf),
            V((heads, length, QK), bf), triangle, triangle,
            V((pairs, length, 512), bf), V((block, width), f32), V((block, ROPE_DIM), f32),
            V(piece, bf), V(piece, bf), V(piece, bf),
            V((pairs, 2, chips, depth, 512), bf), V((pairs, chips, depth, 512), bf),
            V((pairs, chips, depth, 512), bf), V((pairs, chips, depth, 512), bf),
            dma(8), dma(1), dma(1),
            dma(1), dma(pairs), dma(1), dma(pairs),
            dma(1), dma(tiles, pieces), dma(1), dma(tiles, pieces),
            dma(1), dma(pairs), dma(1), dma(pairs),
        ],
        compiler_params=pltpu.CompilerParams(
            collective_id=0, has_side_effects=True, vmem_limit_bytes=50 * 1024 * 1024
        ),
        name="fused_backward",
    )(*(pltpu.with_memory_space_constraint(jnp.asarray(x), pltpu.HBM) for x in (
        latent, rope_t, kv_gain.reshape(1, -1), np.tile(cosine, (1, 4)),
        np.concatenate([-sine, sine, -sine, sine], axis=1),
        np.ascontiguousarray(cosine.T), np.ascontiguousarray(sine.T),
        queries, out_grad, key_up, value_up,
    )))


def write_kernel(dq_ref, grad_ref, low_ref, dq_out, lat_out, rot_out, key_out, value_out, rot, sem):
    count, rows = low_ref.shape[0], lat_out.shape[0] // low_ref.shape[0]
    copies = [
        pltpu.make_async_copy(src, dst_, sem.at[j]) for j, (src, dst_) in enumerate((
            (dq_ref, dq_out), (grad_ref.at[0], key_out), (grad_ref.at[1], value_out), (rot, rot_out)))]
    copies += [
        pltpu.make_async_copy(
            low_ref.at[j, pl.ds(0, rows)], lat_out.at[pl.ds(j * rows, rows)], sem.at[4 + j])
        for j in range(count)]
    for j, copy in enumerate(copies):
        if j != 3:
            copy.start()
    turned = []
    for j in range(count):
        wide = unflat(low_ref[j, rows:].astype(jnp.float32))
        turned += [wide, pltpu.roll(wide, 64, 1)]
    rot[...] = jnp.concatenate(turned, axis=0).T[:ROPE_DIM].astype(jnp.bfloat16)
    copies[3].start()
    for copy in copies:
        copy.wait()


def write(dq, grad, low, length):
    width = low.shape[2]
    bf, f32 = jnp.bfloat16, jnp.float32
    return pl.pallas_call(
        write_kernel,
        in_specs=[pl.BlockSpec(memory_space=pltpu.VMEM)] * 3,
        out_specs=[pl.BlockSpec(memory_space=pl.ANY)] * 5,
        out_shape=[
            jax.ShapeDtypeStruct(dq.shape, bf),
            jax.ShapeDtypeStruct((length, width), bf),
            jax.ShapeDtypeStruct((ROPE_DIM, length), bf),
            jax.ShapeDtypeStruct(grad.shape[1:], f32),
            jax.ShapeDtypeStruct(grad.shape[1:], f32),
        ],
        scratch_shapes=[pltpu.VMEM((ROPE_DIM, length), bf), pltpu.SemaphoreType.DMA((4 + low.shape[0],))],
        compiler_params=pltpu.CompilerParams(vmem_limit_bytes=16 * 1024 * 1024),
        name="write_outputs",
    )(dq, grad, low)


def shards(queries, out_grad, latent, rope_key, kv_gain, key_up, value_up):
    length, width = latent.shape[1:]
    n_sp, n_dp = lax.axis_size("sp"), lax.axis_size("dp")
    grad_scale = float(n_dp * length) ** (-0.5)
    rope_t = jnp.swapaxes(rope_key, 1, 2)[0]
    dq, grad, low = fused(
        queries[0], out_grad[0], latent[0], rope_t, kv_gain, key_up, value_up, grad_scale, n_sp, n_dp
    )
    dq, lat, rot_t, key_grad, value_grad = write(dq, grad, low.reshape(-1, *low.shape[2:]), length)
    return dq[None], lat[None], jnp.swapaxes(rot_t[None], 1, 2), key_grad, value_grad


def solution(mesh):
    return jax.shard_map(
        shards,
        mesh=mesh,
        in_specs=(
            P("dp", None, "sp"),
            P("dp", None, "sp"),
            P("dp", None, None),
            P("dp", None, None),
            P(),
            P("dp", "sp"),
            P("dp", "sp"),
        ),
        out_specs=(
            P("dp", None, "sp"),
            P("dp", None, None),
            P("dp", None, None),
            P("dp", "sp"),
            P("dp", "sp"),
        ),
        check_vma=False,
    )
```
